32 devices in a mesh: fs: 8 (over z, y), tp: 4 (over x, core).
Axes of the slice: x: 2, y: 2, z: 4, core: 2. Of those that a mesh axis runs over, the one named last changes fastest.
Arguments:
- hidden_states: bfloat16 [2048, 2048], P('tp', 'fs'), may hold values from -6 to 6
- norm_gain: float32 [2048], P('fs'), may hold values from 0.1 to 1.9
- gate_master: float32 [8, 2048, 7168], P(None, 'fs', 'tp'), may hold values from -0.125 to 0.125
- up_master: float32 [8, 2048, 7168], P(None, 'fs', 'tp'), may hold values from -0.125 to 0.125
- down_master: float32 [8, 2048, 7168], P(None, 'fs', 'tp'), may hold values from -0.0625 to 0.0625
- expert_ids: int32 [2048, 2], P('tp'), may hold values from 0 to 7, all different within a row; in each aligned block of 512 rows (0 to 511, 512 to 1023, ...) at most 256 rows name the same one
- route_logits: float32 [2048, 2], P('tp'), may hold values from -6 to 6
Outputs:
- gate_serve: bfloat16 [8, 2048, 7168], P('tp', None, 'fs')
- up_serve: bfloat16 [8, 2048, 7168], P('tp', None, 'fs')
- down_serve: bfloat16 [8, 2048, 7168], P('tp', None, 'fs')
- combined: bfloat16 [2048, 2048], P('tp', 'fs')
The draws below stay inside these ranges and needn't reach their ends.
Inputs may be any that keep to these rules, and one draw needn't show every extreme that they name: `expert_ids`: the 2 entries of a row differ. Among the rows of one index of tp (aligned blocks of 512 rows) no expert is named more than 256 times, and in some blocks one expert is named exactly 256 times.
All inputs are finite; a program needn't handle non-finite values.
Results may differ from the reference program's by a relative error of at most 0.018.
Values may be sent and summed in bfloat16 or wider, within the bound.
A program may use at most 192 MiB of HBM per device.

```python
import math
import jax
import jax.numpy as jnp
import numpy as np
from jax import lax

D = 2048
FF = 7168
EXPERTS = 8
TOP = 2
TOK_DEV = 512
CAP = 256
TOKENS = 2048


def levels(key, dims, shards, smallest, largest):
    def one(axis_at, blocks):
        steps = jax.random.uniform(jax.random.fold_in(jax.random.fold_in(key, 6), axis_at), (blocks,), jnp.float32, smallest / len(shards), largest / len(shards))
        return jnp.repeat(jnp.exp(steps), dims[axis_at] // blocks).reshape((-1,) + (1,) * (len(dims) - axis_at - 1))

    loudness = one(*shards[0])
    for cut in shards[1:]:
        loudness = loudness * one(*cut)
    return loudness


def shared_out(key, own, number, rows, amount, top, bound, slope):
    sequence = jax.random.permutation(key, amount)
    heavy_load, ordinary = load_shares(amount, rows * top, bound, slope, True), load_shares(amount, rows * top, bound, slope, False)
    places = jnp.arange(amount)

    def named(lengths, offset_by):
        used = int((lengths > 0).sum())
        fixed = max(1, used // 4)
        passed = fixed + (places - fixed + offset_by * (used - fixed)) % max(1, amount - fixed)
        return jnp.zeros((amount,), jnp.int32).at[sequence[jnp.where(places < fixed, places, passed)]].set(jnp.asarray(lengths, jnp.int32))

    lengths = jnp.where(number % 4 == 0, named(heavy_load, number // 4), named(ordinary, number - number // 4 - 1))
    mixed = jax.random.permutation(jax.random.fold_in(own, 3), amount)
    donor, taker = mixed[0:amount // 2 * 2:2], mixed[1:amount // 2 * 2:2]
    room = jnp.minimum(lengths[donor] - 1, bound - lengths[taker]) // 2
    room = jnp.where((donor == sequence[0]) | (taker == sequence[0]) | (lengths[taker] == 0), 0, jnp.maximum(room, 0))
    passed = jax.random.randint(jax.random.fold_in(own, 4), (amount // 2,), 0, 1 << 20) % (room + 1)
    lengths = lengths.at[donor].add(-passed).at[taker].add(passed)
    labels = jnp.searchsorted(jnp.cumsum(lengths), jnp.arange(rows * top), side="right").astype(jnp.int32)
    listing = labels.reshape(top, rows).T
    listing = listing[jax.random.permutation(jax.random.fold_in(own, 1), rows)]
    offset_by = jax.random.randint(jax.random.fold_in(own, 2), (rows, 1), 0, top)
    return jnp.take_along_axis(listing, (jnp.arange(top)[None, :] + offset_by) % top, axis=1)


def load_shares(amount, total, limit, lean, full):
    loads = [(1 << 20) // math.isqrt(rank ** lean) + 1 for rank in range(1, amount + 1)]
    largest = limit if full else min(limit, max(-(-total // amount), total * loads[0] // sum(loads)))
    least = 1 if total - largest >= amount - 1 else 0
    counts, spare = [largest] + [least] * (amount - 1), total - largest - least * (amount - 1)
    while spare > 0:
        candidates = [i for i in range(1, amount) if counts[i] < largest] or [i for i in range(1, amount) if counts[i] < limit]
        whole, left = sum([loads[i] for i in candidates]), spare
        for i in candidates:
            extra = min(limit - counts[i], max(1, left * loads[i] // whole), spare)
            counts[i] = counts[i] + extra
            spare = spare - extra
    return np.array(counts)


def scatter_about(key, extent, deviation, limit, shards=(), kind=jnp.bfloat16):
    array = deviation * jax.random.normal(key, extent, jnp.float32)
    if shards:
        array = array * levels(key, extent, shards, -0.22, 0.18)
    return jnp.clip(array, -limit, limit).astype(kind)


def setup_inputs(seed: int = 0) -> dict:
    keys = jax.random.split(jax.random.key(seed), 8)
    hidden_states = scatter_about(keys[0], (TOKENS, D), 1.0, 6.0, ((0, 4), (1, 8)))
    norm_gain = jnp.clip(1.0 + 0.18 * jax.random.normal(keys[1], (D,), jnp.float32), 0.1, 1.9)
    gate_master = scatter_about(keys[2], (EXPERTS, D, FF), D ** -0.5, 0.125, ((1, 8), (2, 4)), jnp.float32)
    up_master = scatter_about(keys[3], (EXPERTS, D, FF), D ** -0.5, 0.125, ((1, 8), (2, 4)), jnp.float32)
    down_master = scatter_about(keys[4], (EXPERTS, D, FF), FF ** -0.5, 0.0625, ((1, 8), (2, 4)), jnp.float32)
    expert_ids_keys = jax.random.split(jax.random.fold_in(keys[5], 1), TOKENS // TOK_DEV)
    expert_ids_turns = jax.random.permutation(jax.random.fold_in(keys[5], 3), TOKENS // TOK_DEV)
    expert_ids = jax.vmap(lambda own, number: shared_out(jax.random.fold_in(keys[5], 2), own, number, TOK_DEV, EXPERTS, TOP, CAP, 2))(expert_ids_keys, expert_ids_turns).reshape((TOKENS, TOP))
    route_logits = scatter_about(keys[6], (TOKENS, TOP), 1.0, 6.0, ((0, 4),), jnp.float32)
    return {"hidden_states": hidden_states, "norm_gain": norm_gain, "gate_master": gate_master, "up_master": up_master, "down_master": down_master, "expert_ids": expert_ids, "route_logits": route_logits}


EPSILON = 1e-06

def reference(hidden_states, norm_gain, gate_master, up_master, down_master, expert_ids, route_logits):
    scaled = norm_gain[None, :, None]
    gate_serve = (scaled * gate_master).astype(jnp.bfloat16)
    up_serve = (scaled * up_master).astype(jnp.bfloat16)
    down_serve = down_master.astype(jnp.bfloat16)
    values = hidden_states.astype(jnp.float32)
    inv_rms = lax.rsqrt(lax.optimization_barrier(jnp.mean(values * values, axis=1, keepdims=True)) + EPSILON)
    normed = (values * inv_rms).astype(jnp.bfloat16)
    route_weight = jax.nn.softmax(route_logits, axis=1)

    def expert_output(expert):
        gate_pre = jnp.dot(normed, gate_serve[expert], preferred_element_type=jnp.float32)
        up_pre = jnp.dot(normed, up_serve[expert], preferred_element_type=jnp.float32)
        act = (jax.nn.silu(gate_pre) * up_pre).astype(jnp.bfloat16)
        return jnp.dot(act, down_serve[expert].T, preferred_element_type=jnp.float32).astype(jnp.bfloat16)
    outputs = lax.map(expert_output, jnp.arange(EXPERTS, dtype=jnp.int32))
    by_token = jnp.transpose(outputs, (1, 0, 2))
    picked = jnp.take_along_axis(by_token, expert_ids[:, :, None].astype(jnp.int32), axis=1)
    combined = lax.optimization_barrier(jnp.sum(route_weight[:, :, None] * picked.astype(jnp.float32), axis=1)).astype(jnp.bfloat16)
    return (gate_serve, up_serve, down_serve, combined)
```

```python
import functools

import jax
import jax.numpy as jnp
from jax import lax
from jax.experimental import pallas as pl
from jax.experimental.pallas import tpu as pltpu
from jax.sharding import PartitionSpec as P

EPSILON = 1e-06
SLOTS = 4
MESH = pl.DeviceIdType.MESH


def exchange_kernel(
    groups, row_groups, expert, chunks, gain_ref, gate_ref, up_ref, down_ref, dep_ref,
    gate_out, up_out, down_out, stage, cast, landed, load_sem,
    send_a, recv_a, send_b, recv_b,
):
    me = lax.axis_index("tp")
    row = lax.axis_index("fs")
    blocks = row_groups // groups
    masters = (gate_ref, up_ref, down_ref)
    outs = (gate_out, up_out, down_out)
    local_count = gate_ref.shape[0] // groups
    rows, columns = gate_ref.shape[1:]
    height = rows // chunks
    width = columns // blocks

    barrier = pltpu.get_barrier_semaphore()
    for step in range(1, groups):
        pl.semaphore_signal(
            barrier, inc=1, device_id={"tp": lax.rem(me + step, groups)}, device_id_type=MESH
        )
    for step in range(1, row_groups):
        pl.semaphore_signal(
            barrier, inc=1, device_id={"fs": lax.rem(row + step, row_groups)}, device_id_type=MESH
        )
    order = [groups // 2] + [s for s in range(1, groups) if s != groups // 2] + [0]
    units = [(w, c) for w in range(len(masters)) for c in range(chunks)]
    jobs = [(u, s) for u in range(len(units)) for s in order]

    def load(n):
        u, s = jobs[n]
        w, c = units[u]
        number = lax.rem(me + s, groups) * local_count + expert
        return pltpu.make_async_copy(
            masters[w].at[number, pl.ds(c * height, height)],
            stage.at[n % SLOTS],
            load_sem.at[n % SLOTS],
        )

    for n in range(SLOTS):
        load(n).start()
    pl.semaphore_wait(barrier, groups - 1 + row_groups - 1)

    def first(u, s):
        return pltpu.make_async_remote_copy(
            src_ref=cast.at[u, s],
            dst_ref=landed.at[u, s - 1],
            send_sem=send_a.at[u, s - 1],
            recv_sem=recv_a.at[u, s - 1],
            device_id={"tp": lax.rem(me + s, groups)},
            device_id_type=MESH,
        )

    def place(u, source):
        w, c = units[u]
        start = pl.multiple_of(source * rows + c * height, height)
        return outs[w].at[pl.ds(start, height)]

    def second(u, s, b):
        held = cast.at[u, 0] if s == 0 else landed.at[u, s - 1]
        goal = lax.rem(me + groups - s, groups) * blocks + b
        piece = held.at[:, pl.ds(b * width, width)]
        remote = lambda: pltpu.make_async_remote_copy(
            src_ref=piece,
            dst_ref=place(u, row),
            send_sem=send_b.at[u, s * blocks + b],
            recv_sem=recv_b.at[u, row],
            device_id={"fs": goal},
            device_id_type=MESH,
        )
        local = lambda: pltpu.make_async_copy(piece, place(u, row), recv_b.at[u, row])
        return goal, remote, local

    def pass_on(u, s):
        for b in range(blocks):
            goal, remote, local = second(u, s, b)

            @pl.when(goal != row)
            def _():
                remote().start()

            @pl.when(goal == row)
            def _():
                local().start()

    def forward(u):
        for s in sorted(range(1, groups), key=lambda s: s == groups // 2):
            first(u, s).wait_recv()
            pass_on(u, s)

    strip = 16
    for n, (u, s) in enumerate(jobs):
        w, c = units[u]
        load(n).wait()
        slot = n % SLOTS

        def convert(i, carry):
            at = pl.ds(pl.multiple_of(i * strip, strip), strip)
            value = stage[slot, at, :]
            if w < 2:
                gain = gain_ref[pl.ds(pl.multiple_of(c * height + i * strip, strip), strip), :]
                value = value * gain
            cast[u, s, at, :] = value.astype(jnp.bfloat16)
            return carry

        lax.fori_loop(0, height // strip, convert, 0)
        if n + SLOTS < len(jobs):
            load(n + SLOTS).start()
        if s == 0:
            pass_on(u, 0)
            if u >= 1:
                forward(u - 1)
        else:
            first(u, s).start()
    forward(len(units) - 1)
    for u in range(len(units)):
        for s in range(groups):
            if s:
                first(u, s).wait_send()
            for b in range(blocks):
                goal, remote, local = second(u, s, b)

                @pl.when(goal != row)
                def _():
                    remote().wait_send()
        for source in range(row_groups):
            pltpu.make_async_copy(
                cast.at[u, 0, :, pl.ds(0, width)], place(u, source), recv_b.at[u, source]
            ).wait()


def exchange(gain, gate, up, down, dep, expert, collective):
    groups = lax.axis_size("tp")
    row_groups = lax.axis_size("fs")
    experts, rows, columns = gate.shape
    blocks = row_groups // groups
    width = columns // blocks
    chunks = 2
    units = 3 * chunks
    height = rows // chunks
    out = jax.ShapeDtypeStruct((rows * row_groups, width), jnp.bfloat16)
    hbm = pl.BlockSpec(memory_space=pl.ANY)
    sent = 3 * rows * columns * 2 * groups
    return pl.pallas_call(
        functools.partial(exchange_kernel, groups, row_groups, expert, chunks),
        out_shape=(out, out, out),
        in_specs=[pl.BlockSpec(memory_space=pltpu.VMEM), hbm, hbm, hbm, hbm],
        out_specs=(hbm, hbm, hbm),
        scratch_shapes=[
            pltpu.VMEM((SLOTS, height, columns), jnp.float32),
            pltpu.VMEM((units, groups, height, columns), jnp.bfloat16),
            pltpu.VMEM((units, groups - 1, height, columns), jnp.bfloat16),
            pltpu.SemaphoreType.DMA((SLOTS,)),
            pltpu.SemaphoreType.DMA((units, groups - 1)),
            pltpu.SemaphoreType.DMA((units, groups - 1)),
            pltpu.SemaphoreType.DMA((units, row_groups)),
            pltpu.SemaphoreType.DMA((units, row_groups)),
        ],
        compiler_params=pltpu.CompilerParams(
            collective_id=collective, has_side_effects=True, vmem_limit_bytes=44 * 1024 * 1024
        ),
        cost_estimate=pl.CostEstimate(
            flops=rows * columns, bytes_accessed=32 * sent, transcendentals=0
        ),
    )(gain, gate, up, down, dep)


def serve_kernel(
    groups, row_groups, expert, chunks, gain_ref, gate_ref, up_ref, down_ref, all_ref, spot_ref,
    gate_first, up_first, down_first,
    gate_out, up_out, down_out, early_out, partial_out,
    stage, cast, landed, raw, rows_in, gate_w, up_w, down_w, act, partial, pair, summed, far, total,
    load_sem, send_a, recv_a, send_b, recv_b, raw_sem, weight_sem, keep_sem,
    send_c, recv_c, send_d, recv_d, send_e, recv_e, last_sem,
):
    me = lax.axis_index("tp")
    row = lax.axis_index("fs")
    blocks = row_groups // groups
    masters = (gate_ref, up_ref, down_ref)
    outs = (gate_out, up_out, down_out)
    firsts = (gate_first, up_first, down_first)
    held_w = (gate_w, up_w, down_w)
    local_count = gate_ref.shape[0] // groups
    rows, columns = gate_ref.shape[1:]
    height = rows // chunks
    width = columns // blocks
    tokens, model_width = raw.shape
    capacity = tokens // 2
    side = lax.rem(row, 2)
    mate = row + 1 - 2 * side
    stack = row_groups // 2
    level = row // 2
    strip = 16

    barrier = pltpu.get_barrier_semaphore()
    for step in range(1, groups):
        pl.semaphore_signal(
            barrier, inc=1, device_id={"tp": lax.rem(me + step, groups)}, device_id_type=MESH
        )
    for step in range(1, row_groups):
        pl.semaphore_signal(
            barrier, inc=1, device_id={"fs": lax.rem(row + step, row_groups)}, device_id_type=MESH
        )
    order = [groups // 2] + [s for s in range(1, groups) if s != groups // 2] + [0]
    units = [(w, c) for w in range(len(masters)) for c in range(chunks)]
    jobs = [(u, s) for u in range(len(units)) for s in order]

    def load(n):
        u, s = jobs[n]
        w, c = units[u]
        number = lax.rem(me + s, groups) * local_count + expert
        return pltpu.make_async_copy(
            masters[w].at[number, pl.ds(c * height, height)],
            stage.at[n % SLOTS],
            load_sem.at[n % SLOTS],
        )

    for n in range(SLOTS):
        load(n).start()
    pl.semaphore_wait(barrier, groups - 1 + row_groups - 1)

    def first(u, s):
        return pltpu.make_async_remote_copy(
            src_ref=cast.at[u, s],
            dst_ref=landed.at[u, s - 1],
            send_sem=send_a.at[u, s - 1],
            recv_sem=recv_a.at[u, s - 1],
            device_id={"tp": lax.rem(me + s, groups)},
            device_id_type=MESH,
        )

    def place(u, source):
        w, c = units[u]
        start = pl.multiple_of(source * rows + c * height, height)
        return outs[w].at[expert, pl.ds(start, height)]

    def second(u, s, b):
        held = cast.at[u, 0] if s == 0 else landed.at[u, s - 1]
        goal = lax.rem(me + groups - s, groups) * blocks + b
        piece = held.at[:, pl.ds(b * width, width)]
        remote = lambda: pltpu.make_async_remote_copy(
            src_ref=piece,
            dst_ref=place(u, row),
            send_sem=send_b.at[u, s * blocks + b],
            recv_sem=recv_b.at[u, row],
            device_id={"fs": goal},
            device_id_type=MESH,
        )
        local = lambda: pltpu.make_async_copy(piece, place(u, row), recv_b.at[u, row])
        return goal, remote, local

    def pass_on(u, s):
        for b in range(blocks):
            goal, remote, local = second(u, s, b)

            @pl.when(goal != row)
            def _():
                remote().start()

            @pl.when(goal == row)
            def _():
                local().start()

    def forward(u):
        for s in sorted(range(1, groups), key=lambda s: s == groups // 2):
            first(u, s).wait_recv()
            pass_on(u, s)

    def arrived(u):
        for source in range(row_groups):
            pltpu.make_async_copy(
                cast.at[u, 0, :, pl.ds(0, width)], place(u, source), recv_b.at[u, source]
            ).wait()

    def pack(j):
        def one(g, carry):
            copies = [
                pltpu.make_async_copy(
                    all_ref.at[f, g, pl.ds(0, tokens)],
                    raw.at[:, pl.ds(f * (model_width // row_groups), model_width // row_groups)],
                    raw_sem.at[f],
                )
                for f in range(row_groups)
            ]
            for copy in copies:
                copy.start()
            for copy in copies:
                copy.wait()
            spot = spot_ref[pl.ds(j * groups + g, 1), :]
            slot = lax.broadcasted_iota(jnp.int32, (capacity, tokens), 0)
            table = jnp.where(slot == spot, 1.0, 0.0).astype(jnp.bfloat16)
            packed = jnp.dot(table, raw[...], preferred_element_type=jnp.float32)
            mean = jnp.mean(packed * packed, axis=1, keepdims=True)
            at = pl.ds(pl.multiple_of(g * capacity, capacity), capacity)
            rows_in[at, :] = (packed * lax.rsqrt(mean + EPSILON)).astype(jnp.bfloat16)
            return carry

        lax.fori_loop(0, groups, one, 0)

    def hidden():
        def one(t, carry):
            at = pl.ds(pl.multiple_of(t * capacity, capacity), capacity)
            value = rows_in[at, :]
            gate_pre = jnp.dot(value, gate_w[...], preferred_element_type=jnp.float32)
            up_pre = jnp.dot(value, up_w[...], preferred_element_type=jnp.float32)
            act[at, :] = (gate_pre / (1.0 + jnp.exp(-gate_pre)) * up_pre).astype(jnp.bfloat16)
            return carry

        lax.fori_loop(0, groups, one, 0)

    def lower():
        def one(r, carry):
            at = pl.ds(pl.multiple_of(r * rows, rows), rows)
            partial[at, :] = lax.dot_general(
                down_w[at, :], act[...], (((1,), (1,)), ((), ())), preferred_element_type=jnp.float32
            ).astype(jnp.bfloat16)
            return carry

        lax.fori_loop(0, row_groups, one, 0)

    def fetch(w, j):
        source = firsts[w] if j == 0 else outs[w].at[j]
        return pltpu.make_async_copy(source, held_w[w], weight_sem.at[w])

    def keep(w):
        return pltpu.make_async_copy(held_w[w], outs[w].at[0], keep_sem.at[w])

    levels = [stack // 2] + [k for k in range(1, stack) if k != stack // 2] + [0]

    def rows_of(k, which):
        return (lax.rem(level + k, stack) * 2 + which) * rows

    def across(k):
        return pltpu.make_async_remote_copy(
            src_ref=partial.at[pl.ds(pl.multiple_of(rows_of(k, 1 - side), rows), rows)],
            dst_ref=pair.at[k],
            send_sem=send_c.at[k],
            recv_sem=recv_c.at[k],
            device_id={"fs": mate},
            device_id_type=MESH,
        )

    def along(k):
        return pltpu.make_async_remote_copy(
            src_ref=summed.at[k - 1],
            dst_ref=far.at[k - 1],
            send_sem=send_d.at[k - 1],
            recv_sem=recv_d.at[k - 1],
            device_id={"fs": lax.rem(level + k, stack) * 2 + side},
            device_id_type=MESH,
        )

    def back(s):
        goal = lax.rem(me + s, groups)
        return pltpu.make_async_remote_copy(
            src_ref=total.at[:, pl.ds(pl.multiple_of(goal * capacity, capacity), capacity)],
            dst_ref=early_out.at[me],
            send_sem=send_e.at[s - 1],
            recv_sem=recv_e.at[s - 1],
            device_id={"tp": goal},
            device_id_type=MESH,
        )

    kept = pltpu.make_async_copy(
        total.at[:, pl.ds(pl.multiple_of(me * capacity, capacity), capacity)],
        early_out.at[me],
        last_sem.at[0],
    )

    def own_sum(k, i):
        at = pl.ds(pl.multiple_of(i * strip, strip), strip)
        mine = pl.ds(pl.multiple_of(rows_of(k, side) + i * strip, strip), strip)
        return at, partial[mine, :].astype(jnp.float32) + pair[k, at, :].astype(jnp.float32)

    def after_0():
        for w in range(len(masters)):
            fetch(w, 0).start()
        pack(0)

    def after_1():
        for w in range(2):
            fetch(w, 0).wait()
            keep(w).start()
        hidden()

    def after_2():
        fetch(2, 0).wait()
        keep(2).start()
        lower()
        for k in levels:
            across(k).start()

    def after_3():
        for k in levels:
            across(k).wait_recv()
            if k:

                def add(i, carry):
                    at, both = own_sum(k, i)
                    summed[k - 1, at, :] = both.astype(jnp.bfloat16)
                    return carry

                lax.fori_loop(0, rows // strip, add, 0)
                along(k).start()

    def after_4():
        for k in range(1, stack):
            along(k).wait_recv()

        def finish(i, carry):
            at, value = own_sum(0, i)
            for k in range(1, stack):
                value = value + far[k - 1, at, :].astype(jnp.float32)
            total[at, :] = value.astype(jnp.bfloat16)
            return carry

        lax.fori_loop(0, rows // strip, finish, 0)
        for s in range(1, groups):
            back(s).start()
        kept.start()

    tasks = {0: after_0, 1: after_1, 2: after_2, 3: after_3}

    for n, (u, s) in enumerate(jobs):
        w, c = units[u]
        load(n).wait()
        slot = n % SLOTS

        def convert(i, carry):
            at = pl.ds(pl.multiple_of(i * strip, strip), strip)
            value = stage[slot, at, :]
            if w < 2:
                gain = gain_ref[pl.ds(pl.multiple_of(c * height + i * strip, strip), strip), :]
                value = value * gain
            cast[u, s, at, :] = value.astype(jnp.bfloat16)
            return carry

        lax.fori_loop(0, height // strip, convert, 0)
        if n + SLOTS < len(jobs):
            load(n + SLOTS).start()
        if s == 0:
            pass_on(u, 0)
            if u >= 1:
                forward(u - 1)
            if u in tasks:
                tasks[u]()
        else:
            first(u, s).start()
    forward(len(units) - 1)
    pack(1)
    for k in range(stack):
        across(k).wait_send()
    after_4()
    for w in range(2):
        keep(w).wait()
        for c in range(chunks):
            arrived(w * chunks + c)
        fetch(w, expert).start()
    for w in range(2):
        fetch(w, expert).wait()
    hidden()
    keep(2).wait()
    for c in range(chunks):
        arrived(2 * chunks + c)
    fetch(2, expert).start()
    fetch(2, expert).wait()
    lower()
    done = pltpu.make_async_copy(partial, partial_out, last_sem.at[1])
    done.start()
    kept.wait()
    for s in range(1, groups):
        back(s).wait()
    for k in range(1, stack):
        along(k).wait_send()
    for u in range(len(units)):
        for s in range(groups):
            if s:
                first(u, s).wait_send()
            for b in range(blocks):
                goal, remote, local = second(u, s, b)

                @pl.when(goal != row)
                def _():
                    remote().wait_send()
    done.wait()


def serve(gain, gate, up, down, everything, spots, firsts, expert, collective):
    groups = lax.axis_size("tp")
    row_groups = lax.axis_size("fs")
    experts, rows, columns = gate.shape
    blocks = row_groups // groups
    width = columns // blocks
    model_width = rows * row_groups
    tokens = spots.shape[1]
    capacity = tokens // 2
    slots = groups * capacity
    chunks = 2
    units = 3 * chunks
    height = rows // chunks
    stack = row_groups // 2
    out = jax.ShapeDtypeStruct((experts // groups, model_width, width), jnp.bfloat16)
    hbm = pl.BlockSpec(memory_space=pl.ANY)
    vmem = pl.BlockSpec(memory_space=pltpu.VMEM)
    sent = 3 * rows * columns * 2 * groups
    weight = pltpu.VMEM((model_width, width), jnp.bfloat16)
    dma = lambda *shape: pltpu.SemaphoreType.DMA(shape)
    return pl.pallas_call(
        functools.partial(serve_kernel, groups, row_groups, expert, chunks),
        out_shape=(
            out, out, out,
            jax.ShapeDtypeStruct((groups, rows, capacity), jnp.bfloat16),
            jax.ShapeDtypeStruct((model_width, slots), jnp.bfloat16),
        ),
        in_specs=[vmem, hbm, hbm, hbm, hbm, vmem, hbm, hbm, hbm],
        out_specs=(hbm,) * 5,
        scratch_shapes=[
            pltpu.VMEM((SLOTS, height, columns), jnp.float32),
            pltpu.VMEM((units, groups, height, columns), jnp.bfloat16),
            pltpu.VMEM((units, groups - 1, height, columns), jnp.bfloat16),
            pltpu.VMEM((tokens, model_width), jnp.bfloat16),
            pltpu.VMEM((slots, model_width), jnp.bfloat16),
            weight, weight, weight,
            pltpu.VMEM((slots, width), jnp.bfloat16),
            pltpu.VMEM((model_width, slots), jnp.bfloat16),
            pltpu.VMEM((stack, rows, slots), jnp.bfloat16),
            pltpu.VMEM((stack - 1, rows, slots), jnp.bfloat16),
            pltpu.VMEM((stack - 1, rows, slots), jnp.bfloat16),
            pltpu.VMEM((rows, slots), jnp.bfloat16),
            dma(SLOTS), dma(units, groups - 1), dma(units, groups - 1),
            dma(units, row_groups), dma(units, row_groups),
            dma(row_groups), dma(3), dma(3),
            dma(stack), dma(stack), dma(stack - 1), dma(stack - 1),
            dma(groups - 1), dma(groups - 1), dma(2),
        ],
        compiler_params=pltpu.CompilerParams(
            collective_id=collective, has_side_effects=True, vmem_limit_bytes=62 * 1024 * 1024
        ),
        cost_estimate=pl.CostEstimate(
            flops=12 * slots * model_width * width, bytes_accessed=32 * sent, transcendentals=0
        ),
    )(gain, gate, up, down, everything, spots, *firsts)


def gather_sum_kernel(
    groups, row_groups, partial_ref, out_ref, own, pair, summed, far, total,
    load_sem, send_a, recv_a, send_b, recv_b, send_c, recv_c,
):
    me = lax.axis_index("tp")
    row = lax.axis_index("fs")
    side = lax.rem(row, 2)
    mate = row + 1 - 2 * side
    stack = row_groups // 2
    level = row // 2
    pieces, slots = total.shape
    capacity = slots // groups

    barrier = pltpu.get_barrier_semaphore()
    for step in range(1, groups):
        pl.semaphore_signal(
            barrier, inc=1, device_id={"tp": lax.rem(me + step, groups)}, device_id_type=MESH
        )
    for step in range(1, row_groups):
        pl.semaphore_signal(
            barrier, inc=1, device_id={"fs": lax.rem(row + step, row_groups)}, device_id_type=MESH
        )
    order = [stack // 2] + [k for k in range(1, stack) if k != stack // 2] + [0]

    def rows_of(k, which):
        goal = lax.rem(level + k, stack) * 2 + which
        return partial_ref.at[pl.ds(pl.multiple_of(goal * pieces, pieces), pieces)]

    def load(k):
        return pltpu.make_async_copy(rows_of(k, side), own.at[k], load_sem.at[k])

    def across(k):
        return pltpu.make_async_remote_copy(
            src_ref=rows_of(k, 1 - side),
            dst_ref=pair.at[k],
            send_sem=send_a.at[k],
            recv_sem=recv_a.at[k],
            device_id={"fs": mate},
            device_id_type=MESH,
        )

    def along(k):
        return pltpu.make_async_remote_copy(
            src_ref=summed.at[k],
            dst_ref=far.at[k],
            send_sem=send_b.at[k],
            recv_sem=recv_b.at[k],
            device_id={"fs": lax.rem(level + k, stack) * 2 + side},
            device_id_type=MESH,
        )

    def back(s):
        goal = lax.rem(me + s, groups)
        columns = pl.ds(pl.multiple_of(goal * capacity, capacity), capacity)
        return pltpu.make_async_remote_copy(
            src_ref=total.at[:, columns],
            dst_ref=out_ref.at[me],
            send_sem=send_c.at[s - 1],
            recv_sem=recv_c.at[s - 1],
            device_id={"tp": goal},
            device_id_type=MESH,
        )

    for k in order:
        load(k).start()
    pl.semaphore_wait(barrier, groups - 1 + row_groups - 1)
    for k in order:
        across(k).start()
    strip = 16
    for k in order:
        load(k).wait()
        across(k).wait_recv()

        def add(i, carry):
            at = pl.ds(pl.multiple_of(i * strip, strip), strip)
            both = own[k, at, :].astype(jnp.float32) + pair[k, at, :].astype(jnp.float32)
            summed[k, at, :] = both.astype(jnp.bfloat16)
            return carry

        if k:
            lax.fori_loop(0, pieces // strip, add, 0)
            along(k).start()
    for k in range(1, stack):
        along(k).wait_recv()

    def finish(i, carry):
        at = pl.ds(pl.multiple_of(i * strip, strip), strip)
        value = own[0, at, :].astype(jnp.float32) + pair[0, at, :].astype(jnp.float32)
        for k in range(1, stack):
            value = value + far[k, at, :].astype(jnp.float32)
        total[at, :] = value.astype(jnp.bfloat16)
        return carry

    lax.fori_loop(0, pieces // strip, finish, 0)
    for s in range(1, groups):
        back(s).start()
    columns = pl.ds(pl.multiple_of(me * capacity, capacity), capacity)
    kept = pltpu.make_async_copy(total.at[:, columns], out_ref.at[me], load_sem.at[0])
    kept.start()
    kept.wait()
    for s in range(1, groups):
        back(s).wait()
    for k in range(stack):
        across(k).wait_send()
        if k:
            along(k).wait_send()


def gather_sum(partial, collective):
    groups = lax.axis_size("tp")
    row_groups = lax.axis_size("fs")
    model_width, slots = partial.shape
    pieces = model_width // row_groups
    stack = row_groups // 2
    capacity = slots // groups
    block = pltpu.VMEM((stack, pieces, slots), jnp.bfloat16)
    sent = model_width * slots * 2
    return pl.pallas_call(
        functools.partial(gather_sum_kernel, groups, row_groups),
        out_shape=jax.ShapeDtypeStruct((groups, pieces, capacity), jnp.bfloat16),
        in_specs=[pl.BlockSpec(memory_space=pl.ANY)],
        out_specs=pl.BlockSpec(memory_space=pl.ANY),
        scratch_shapes=[
            block, block, block, block,
            pltpu.VMEM((pieces, slots), jnp.bfloat16),
            pltpu.SemaphoreType.DMA((stack,)),
            pltpu.SemaphoreType.DMA((stack,)),
            pltpu.SemaphoreType.DMA((stack,)),
            pltpu.SemaphoreType.DMA((stack,)),
            pltpu.SemaphoreType.DMA((stack,)),
            pltpu.SemaphoreType.DMA((groups - 1,)),
            pltpu.SemaphoreType.DMA((groups - 1,)),
        ],
        compiler_params=pltpu.CompilerParams(
            collective_id=collective, has_side_effects=True, vmem_limit_bytes=20 * 1024 * 1024
        ),
        cost_estimate=pl.CostEstimate(
            flops=sent, bytes_accessed=32 * sent, transcendentals=0
        ),
    )(partial)


def fused_device(
    hidden_states, norm_gain, gate_master, up_master, down_master, expert_ids, route_logits
):
    groups = lax.axis_size("tp")
    row_groups = lax.axis_size("fs")
    experts = gate_master.shape[0]
    local_count = experts // groups
    tokens, pieces = hidden_states.shape
    model_width = pieces * row_groups
    capacity = tokens // 2
    me = lax.axis_index("tp")
    gain = norm_gain[:, None]
    id_rows = expert_ids.size // pieces
    sheet = expert_ids.astype(jnp.bfloat16).reshape(id_rows, pieces)
    sheet = jnp.pad(sheet, ((0, -id_rows % 16), (0, 0)))
    everything = lax.all_gather(jnp.concatenate([hidden_states, sheet]), ("fs", "tp"), axis=0)
    everything = everything.reshape(row_groups, groups, -1, pieces)
    all_ids = everything[0, :, tokens : tokens + id_rows].astype(jnp.int32)
    all_ids = all_ids.reshape(groups, tokens, 2)
    earlier = (jnp.arange(tokens)[:, None] > jnp.arange(tokens)[None, :]).astype(jnp.bfloat16)
    weights = jax.nn.softmax(route_logits, axis=1)
    named = expert_ids[:, :, None] == jnp.arange(experts, dtype=jnp.int32)[None, None, :]
    chosen = jnp.any(named, axis=1).astype(jnp.bfloat16)
    before = jnp.dot(earlier, chosen, preferred_element_type=jnp.float32)
    position = jnp.sum(jnp.where(named, before[:, None, :], 0.0), axis=2).astype(jnp.int32)
    slot_ids = (expert_ids * capacity + position).reshape(-1)

    mine = jnp.any(
        all_ids[None] == (me * local_count + jnp.arange(local_count))[:, None, None, None], axis=3
    )
    spots = jnp.einsum(
        "ts,jgs->jgt", earlier, mine.astype(jnp.bfloat16), preferred_element_type=jnp.float32
    ).astype(jnp.int32)
    spots = jnp.where(mine, spots, -1).reshape(local_count * groups, tokens)
    firsts = exchange(gain, gate_master, up_master, down_master, hidden_states, 0, 1)
    gate, up, down, early, partial = serve(
        gain, gate_master, up_master, down_master, everything, spots, firsts, 1, 2
    )
    last = gather_sum(partial, 3)
    ordered = jnp.stack([early, last], axis=1)
    flat_out = jnp.moveaxis(ordered, 2, 0).reshape(pieces, experts * capacity)
    picked = flat_out.at[:, slot_ids].get(mode="promise_in_bounds")
    picked = picked.reshape(pieces, tokens, 2).astype(jnp.float32)
    combined = jnp.sum(picked * weights[None, :, :], axis=2)
    return gate, up, down, jnp.transpose(combined).astype(jnp.bfloat16)


def arrange(weights, groups, row_groups):
    experts, rows, columns = weights.shape
    blocks = row_groups // groups
    split = weights.reshape(experts // groups, groups, rows, blocks, columns // blocks)
    split = split.reshape(groups, experts // groups, rows, blocks, columns // blocks)
    return jnp.transpose(split, (0, 3, 1, 2, 4))


def regroup(moved, row_groups):
    return moved.reshape((row_groups,) + moved.shape[2:])


def settle(arrived):
    return arrived.reshape(arrived.shape[1], arrived.shape[2], arrived.shape[3])


def per_device(
    hidden_states, norm_gain, gate_master, up_master, down_master, expert_ids, route_logits
):
    groups = lax.axis_size("tp")
    row_groups = lax.axis_size("fs")
    whole_tiles = gate_master.shape[2] // (row_groups // groups) % 128 == 0
    if whole_tiles and gate_master.shape[0] == 2 * groups and row_groups % 4 == 0 and expert_ids.size % hidden_states.shape[1] == 0:
        return fused_device(
            hidden_states, norm_gain, gate_master, up_master, down_master, expert_ids, route_logits
        )
    experts = gate_master.shape[0]
    local_count = experts // groups
    tokens = hidden_states.shape[0]
    pieces = hidden_states.shape[1]
    model_width = pieces * row_groups
    capacity = tokens // 2
    scaled = norm_gain[None, :, None]
    gate_cast = arrange((scaled * gate_master).astype(jnp.bfloat16), groups, row_groups)
    up_cast = arrange((scaled * up_master).astype(jnp.bfloat16), groups, row_groups)
    down_cast = arrange(down_master.astype(jnp.bfloat16), groups, row_groups)
    sectioned = (
        lax.all_to_all(gate_cast, "tp", split_axis=0, concat_axis=0, tiled=True),
        lax.all_to_all(up_cast, "tp", split_axis=0, concat_axis=0, tiled=True),
        lax.all_to_all(down_cast, "tp", split_axis=0, concat_axis=0, tiled=True),
    )
    landed = (
        lax.all_to_all(
            regroup(sectioned[0], row_groups), "fs", split_axis=0, concat_axis=2, tiled=True
        ),
        lax.all_to_all(
            regroup(sectioned[1], row_groups), "fs", split_axis=0, concat_axis=2, tiled=True
        ),
        lax.all_to_all(
            regroup(sectioned[2], row_groups), "fs", split_axis=0, concat_axis=2, tiled=True
        ),
    )
    gate_serve, up_serve, down_serve = (settle(landed[0]), settle(landed[1]), settle(landed[2]))
    values = hidden_states.astype(jnp.float32)
    squares = lax.psum(jnp.sum(values * values, axis=1), "fs")
    normed = (values * lax.rsqrt(squares / model_width + EPSILON)[:, None]).astype(jnp.bfloat16)
    weights = jax.nn.softmax(route_logits, axis=1)
    chosen = (expert_ids[:, :, None] == jnp.arange(experts, dtype=jnp.int32)[None, None, :]).astype(
        jnp.int32
    )
    chosen = chosen.reshape(tokens * 2, experts)
    before = jnp.cumsum(chosen, axis=0) - chosen
    position = jnp.sum(before * chosen, axis=1)
    slot_ids = expert_ids.reshape(-1) * capacity + position
    slot_table = (
        slot_ids[None, :] == jnp.arange(experts * capacity, dtype=jnp.int32)[:, None]
    ).astype(jnp.bfloat16)
    dispatch = jnp.sum(slot_table.reshape(experts * capacity, tokens, 2), axis=2)
    whole_rows = lax.all_gather(normed, "fs", axis=1, tiled=True)
    packed = jnp.dot(dispatch, whole_rows, preferred_element_type=jnp.float32).astype(jnp.bfloat16)
    arrived = lax.all_to_all(
        packed.reshape(groups, local_count * capacity, model_width),
        "tp",
        split_axis=0,
        concat_axis=0,
        tiled=True,
    )
    arranged = arrived.reshape(groups, local_count, capacity, model_width)
    activations = []
    for expert_index in range(local_count):
        expert_rows = arranged[:, expert_index].reshape(groups * capacity, model_width)
        gate_pre = jnp.dot(
            expert_rows, gate_serve[expert_index], preferred_element_type=jnp.float32
        )
        up_pre = jnp.dot(expert_rows, up_serve[expert_index], preferred_element_type=jnp.float32)
        activations.append((jax.nn.silu(gate_pre) * up_pre).astype(jnp.bfloat16))
    stacked = jnp.stack(activations)
    summed = lax.psum_scatter(
        jnp.einsum("jdh,jsh->djs", down_serve, stacked, preferred_element_type=jnp.float32).astype(
            jnp.bfloat16
        ),
        "fs",
        scatter_dimension=0,
        tiled=True,
    )
    results = summed.reshape(pieces, local_count, groups, capacity)
    returned = lax.all_to_all(results, "tp", split_axis=2, concat_axis=1, tiled=True)
    flat_out = returned.reshape(pieces, experts * capacity)
    picked = jnp.take(flat_out, slot_ids, axis=1).reshape(pieces, tokens, 2).astype(jnp.float32)
    combined = jnp.sum(picked * weights[None, :, :], axis=2)
    return (gate_serve, up_serve, down_serve, jnp.transpose(combined).astype(jnp.bfloat16))


def solution(mesh):
    in_specs = (
        P("tp", "fs"),
        P("fs"),
        P(None, "fs", "tp"),
        P(None, "fs", "tp"),
        P(None, "fs", "tp"),
        P("tp", None),
        P("tp", None),
    )
    out_specs = (P("tp", None, "fs"), P("tp", None, "fs"), P("tp", None, "fs"), P("tp", "fs"))
    return jax.shard_map(
        per_device, mesh=mesh, in_specs=in_specs, out_specs=out_specs, check_vma=False
    )
```

```python
import functools

import jax
import jax.numpy as jnp
from jax import lax
from jax.experimental import pallas as pl
from jax.experimental.pallas import tpu as pltpu
from jax.sharding import PartitionSpec as P

EPSILON = 1e-06
SLOTS = 4
MESH = pl.DeviceIdType.MESH


def exchange_kernel(
    groups, row_groups, expert, chunks, gain_ref, gate_ref, up_ref, down_ref, own_ref, spot_ref,
    gate_out, up_out, down_out, all_out, spot_out, stage, cast, landed, load_sem,
    send_a, recv_a, send_b, recv_b, send_z, recv_z, send_y, recv_y, send_t, recv_t,
    send_s, recv_s, own_sem,
):
    me = lax.axis_index("tp")
    row = lax.axis_index("fs")
    blocks = row_groups // groups
    masters = (gate_ref, up_ref, down_ref)
    outs = (gate_out, up_out, down_out)
    local_count = gate_ref.shape[0] // groups
    rows, columns = gate_ref.shape[1:]
    height = rows // chunks
    width = columns // blocks

    barrier = pltpu.get_barrier_semaphore()
    for step in range(1, groups):
        pl.semaphore_signal(
            barrier, inc=1, device_id={"tp": lax.rem(me + step, groups)}, device_id_type=MESH
        )
    for step in range(1, row_groups):
        pl.semaphore_signal(
            barrier, inc=1, device_id={"fs": lax.rem(row + step, row_groups)}, device_id_type=MESH
        )
    order = [groups // 2] + [s for s in range(1, groups) if s != groups // 2] + [0]
    units = [(w, c) for w in range(len(masters)) for c in range(chunks)]
    jobs = [(u, s) for u in range(len(units)) for s in order]

    def load(n):
        u, s = jobs[n]
        w, c = units[u]
        number = lax.rem(me + s, groups) * local_count + expert
        return pltpu.make_async_copy(
            masters[w].at[number, pl.ds(c * height, height)],
            stage.at[n % SLOTS],
            load_sem.at[n % SLOTS],
        )

    for n in range(SLOTS):
        load(n).start()
    pl.semaphore_wait(barrier, groups - 1 + row_groups - 1)

    def first(u, s):
        return pltpu.make_async_remote_copy(
            src_ref=cast.at[u, s],
            dst_ref=landed.at[u, s - 1],
            send_sem=send_a.at[u, s - 1],
            recv_sem=recv_a.at[u, s - 1],
            device_id={"tp": lax.rem(me + s, groups)},
            device_id_type=MESH,
        )

    def place(u, source):
        w, c = units[u]
        start = pl.multiple_of(source * rows + c * height, height)
        return outs[w].at[pl.ds(start, height)]

    def second(u, s, b):
        held = cast.at[u, 0] if s == 0 else landed.at[u, s - 1]
        goal = lax.rem(me + groups - s, groups) * blocks + b
        piece = held.at[:, pl.ds(b * width, width)]
        remote = lambda: pltpu.make_async_remote_copy(
            src_ref=piece,
            dst_ref=place(u, row),
            send_sem=send_b.at[u, s * blocks + b],
            recv_sem=recv_b.at[u, row],
            device_id={"fs": goal},
            device_id_type=MESH,
        )
        local = lambda: pltpu.make_async_copy(piece, place(u, row), recv_b.at[u, row])
        return goal, remote, local

    def pass_on(u, s):
        for b in range(blocks):
            goal, remote, local = second(u, s, b)

            @pl.when(goal != row)
            def _():
                remote().start()

            @pl.when(goal == row)
            def _():
                local().start()

    def forward(u):
        for s in sorted(range(1, groups), key=lambda s: s == groups // 2):
            first(u, s).wait_recv()
            pass_on(u, s)

    side = lax.rem(row, 2)
    mate = row + 1 - 2 * side
    stack = row_groups // 2
    level = row // 2

    def block(k, y):
        which = side if y == 0 else 1 - side
        return lax.rem(level + stack - k, stack) * 2 + which

    def up_z(k):
        return pltpu.make_async_remote_copy(
            src_ref=own_ref,
            dst_ref=all_out.at[row, me],
            send_sem=send_z.at[k - 1],
            recv_sem=recv_z.at[k - 1],
            device_id={"fs": lax.rem(level + k, stack) * 2 + side},
            device_id_type=MESH,
        )

    def over_y(k):
        place = all_out.at[block(k, 0), me]
        return pltpu.make_async_remote_copy(
            src_ref=own_ref if k == 0 else place,
            dst_ref=place,
            send_sem=send_y.at[k],
            recv_sem=recv_y.at[k],
            device_id={"fs": mate},
            device_id_type=MESH,
        )

    def over_tp(k, y, s):
        place = all_out.at[block(k, y), me]
        return pltpu.make_async_remote_copy(
            src_ref=own_ref if k == 0 and y == 0 else place,
            dst_ref=place,
            send_sem=send_t.at[y * stack + k, s - 1],
            recv_sem=recv_t.at[y * stack + k, s - 1],
            device_id={"tp": lax.rem(me + s, groups)},
            device_id_type=MESH,
        )

    def spots_to(s):
        goal = lax.rem(me + s, groups)
        return pltpu.make_async_remote_copy(
            src_ref=spot_ref.at[goal],
            dst_ref=spot_out.at[me],
            send_sem=send_s.at[s - 1],
            recv_sem=recv_s.at[s - 1],
            device_id={"tp": goal},
            device_id_type=MESH,
        )

    own_kept = pltpu.make_async_copy(own_ref, all_out.at[row, me], own_sem.at[0])
    spot_kept = pltpu.make_async_copy(spot_ref.at[me], spot_out.at[me], own_sem.at[1])
    own_kept.start()
    spot_kept.start()
    for k in range(1, stack):
        up_z(k).start()
    over_y(0).start()
    for s in range(1, groups):
        spots_to(s).start()

    def near_blocks():
        for k in range(stack):
            if k:
                up_z(k).wait_recv()
                over_y(k).start()
            for s in range(1, groups):
                over_tp(k, 0, s).start()

    def far_blocks():
        for k in range(stack):
            over_y(k).wait_recv()
            for s in range(1, groups):
                over_tp(k, 1, s).start()

    tasks = {1: near_blocks, 3: far_blocks}
    strip = 16
    for n, (u, s) in enumerate(jobs):
        w, c = units[u]
        load(n).wait()
        slot = n % SLOTS

        def convert(i, carry):
            at = pl.ds(pl.multiple_of(i * strip, strip), strip)
            value = stage[slot, at, :]
            if w < 2:
                gain = gain_ref[pl.ds(pl.multiple_of(c * height + i * strip, strip), strip), :]
                value = value * gain
            cast[u, s, at, :] = value.astype(jnp.bfloat16)
            return carry

        lax.fori_loop(0, height // strip, convert, 0)
        if n + SLOTS < len(jobs):
            load(n + SLOTS).start()
        if s == 0:
            pass_on(u, 0)
            if u >= 1:
                forward(u - 1)
            if u in tasks:
                tasks[u]()
        else:
            first(u, s).start()
    forward(len(units) - 1)
    own_kept.wait()
    spot_kept.wait()
    for k in range(stack):
        if k:
            up_z(k).wait_send()
        over_y(k).wait_send()
        for s in range(1, groups):
            for y in range(2):
                over_tp(k, y, s).wait()
    for s in range(1, groups):
        spots_to(s).wait()
    for u in range(len(units)):
        for s in range(groups):
            if s:
                first(u, s).wait_send()
            for b in range(blocks):
                goal, remote, local = second(u, s, b)

                @pl.when(goal != row)
                def _():
                    remote().wait_send()
        for source in range(row_groups):
            pltpu.make_async_copy(
                cast.at[u, 0, :, pl.ds(0, width)], place(u, source), recv_b.at[u, source]
            ).wait()


def exchange(gain, gate, up, down, hidden, spots, expert, collective):
    groups = lax.axis_size("tp")
    row_groups = lax.axis_size("fs")
    experts, rows, columns = gate.shape
    blocks = row_groups // groups
    width = columns // blocks
    chunks = 2
    units = 3 * chunks
    height = rows // chunks
    out = jax.ShapeDtypeStruct((rows * row_groups, width), jnp.bfloat16)
    hbm = pl.BlockSpec(memory_space=pl.ANY)
    stack = row_groups // 2
    vmem = pl.BlockSpec(memory_space=pltpu.VMEM)
    sent = 3 * rows * columns * 2 * groups
    dma = lambda *shape: pltpu.SemaphoreType.DMA(shape)
    return pl.pallas_call(
        functools.partial(exchange_kernel, groups, row_groups, expert, chunks),
        out_shape=(
            out, out, out,
            jax.ShapeDtypeStruct((row_groups, groups) + hidden.shape, hidden.dtype),
            jax.ShapeDtypeStruct(spots.shape, spots.dtype),
        ),
        in_specs=[vmem, hbm, hbm, hbm, vmem, vmem],
        out_specs=(hbm,) * 5,
        scratch_shapes=[
            pltpu.VMEM((SLOTS, height, columns), jnp.float32),
            pltpu.VMEM((units, groups, height, columns), jnp.bfloat16),
            pltpu.VMEM((units, groups - 1, height, columns), jnp.bfloat16),
            dma(SLOTS), dma(units, groups - 1), dma(units, groups - 1),
            dma(units, row_groups), dma(units, row_groups),
            dma(stack - 1), dma(stack - 1), dma(stack), dma(stack),
            dma(2 * stack, groups - 1), dma(2 * stack, groups - 1),
            dma(groups - 1), dma(groups - 1), dma(2),
        ],
        compiler_params=pltpu.CompilerParams(
            collective_id=collective, has_side_effects=True, vmem_limit_bytes=44 * 1024 * 1024
        ),
        cost_estimate=pl.CostEstimate(
            flops=rows * columns, bytes_accessed=32 * sent, transcendentals=0
        ),
    )(gain, gate, up, down, hidden, spots)


def serve_kernel(
    groups, row_groups, expert, chunks, gain_ref, gate_ref, up_ref, down_ref, all_ref, spot_ref,
    gate_first, up_first, down_first,
    gate_out, up_out, down_out, back_out,
    stage, cast, landed, raw, rows_in, gate_w, up_w, down_w, act, partial,
    pair, to_near, near, to_far, far, total,
    load_sem, send_a, recv_a, send_b, recv_b, raw_sem, weight_sem, keep_sem,
    send_c, recv_c, send_d, recv_d, send_f, recv_f, send_e, recv_e, last_sem,
):
    me = lax.axis_index("tp")
    row = lax.axis_index("fs")
    blocks = row_groups // groups
    masters = (gate_ref, up_ref, down_ref)
    outs = (gate_out, up_out, down_out)
    firsts = (gate_first, up_first, down_first)
    held_w = (gate_w, up_w, down_w)
    local_count = gate_ref.shape[0] // groups
    rows, columns = gate_ref.shape[1:]
    height = rows // chunks
    width = columns // blocks
    tokens, model_width = raw.shape
    capacity = tokens // 2
    side = lax.rem(row, 2)
    mate = row + 1 - 2 * side
    stack = row_groups // 2
    level = row // 2
    strip = 16

    barrier = pltpu.get_barrier_semaphore()
    for step in range(1, groups):
        pl.semaphore_signal(
            barrier, inc=1, device_id={"tp": lax.rem(me + step, groups)}, device_id_type=MESH
        )
    for step in range(1, row_groups):
        pl.semaphore_signal(
            barrier, inc=1, device_id={"fs": lax.rem(row + step, row_groups)}, device_id_type=MESH
        )
    order = [groups // 2] + [s for s in range(1, groups) if s != groups // 2] + [0]
    units = [(w, c) for w in range(len(masters)) for c in range(chunks)]
    jobs = [(u, s) for u in range(len(units)) for s in order]

    def load(n):
        u, s = jobs[n]
        w, c = units[u]
        number = lax.rem(me + s, groups) * local_count + expert
        return pltpu.make_async_copy(
            masters[w].at[number, pl.ds(c * height, height)],
            stage.at[n % SLOTS],
            load_sem.at[n % SLOTS],
        )

    for n in range(SLOTS):
        load(n).start()
    pl.semaphore_wait(barrier, groups - 1 + row_groups - 1)

    def first(u, s):
        return pltpu.make_async_remote_copy(
            src_ref=cast.at[u, s],
            dst_ref=landed.at[u, s - 1],
            send_sem=send_a.at[u, s - 1],
            recv_sem=recv_a.at[u, s - 1],
            device_id={"tp": lax.rem(me + s, groups)},
            device_id_type=MESH,
        )

    def place(u, source):
        w, c = units[u]
        start = pl.multiple_of(source * rows + c * height, height)
        return outs[w].at[expert, pl.ds(start, height)]

    def second(u, s, b):
        held = cast.at[u, 0] if s == 0 else landed.at[u, s - 1]
        goal = lax.rem(me + groups - s, groups) * blocks + b
        piece = held.at[:, pl.ds(b * width, width)]
        remote = lambda: pltpu.make_async_remote_copy(
            src_ref=piece,
            dst_ref=place(u, row),
            send_sem=send_b.at[u, s * blocks + b],
            recv_sem=recv_b.at[u, row],
            device_id={"fs": goal},
            device_id_type=MESH,
        )
        local = lambda: pltpu.make_async_copy(piece, place(u, row), recv_b.at[u, row])
        return goal, remote, local

    def pass_on(u, s):
        for b in range(blocks):
            goal, remote, local = second(u, s, b)

            @pl.when(goal != row)
            def _():
                remote().start()

            @pl.when(goal == row)
            def _():
                local().start()

    def forward(u):
        for s in sorted(range(1, groups), key=lambda s: s == groups // 2):
            first(u, s).wait_recv()
            pass_on(u, s)

    def arrived(u, source):
        pltpu.make_async_copy(
            cast.at[u, 0, :, pl.ds(0, width)], place(u, source), recv_b.at[u, source]
        ).wait()

    def pack(j):
        def one(g, carry):
            copies = [
                pltpu.make_async_copy(
                    all_ref.at[f, g],
                    raw.at[:, pl.ds(f * (model_width // row_groups), model_width // row_groups)],
                    raw_sem.at[f],
                )
                for f in range(row_groups)
            ]
            for copy in copies:
                copy.start()
            for copy in copies:
                copy.wait()
            spot = spot_ref[g, pl.ds(j, 1), :]
            slot = lax.broadcasted_iota(jnp.int32, (capacity, tokens), 0).astype(jnp.float32)
            table = jnp.where(slot == spot, 1.0, 0.0).astype(jnp.bfloat16)
            packed = jnp.dot(table, raw[...], preferred_element_type=jnp.float32)
            mean = jnp.mean(packed * packed, axis=1, keepdims=True)
            at = pl.ds(pl.multiple_of(g * capacity, capacity), capacity)
            rows_in[at, :] = (packed * lax.rsqrt(mean + EPSILON)).astype(jnp.bfloat16)
            return carry

        lax.fori_loop(0, groups, one, 0)

    def hidden():
        def one(t, carry):
            at = pl.ds(pl.multiple_of(t * capacity, capacity), capacity)
            value = rows_in[at, :]
            gate_pre = jnp.dot(value, gate_w[...], preferred_element_type=jnp.float32)
            up_pre = jnp.dot(value, up_w[...], preferred_element_type=jnp.float32)
            act[at, :] = (gate_pre / (1.0 + jnp.exp(-gate_pre)) * up_pre).astype(jnp.bfloat16)
            return carry

        lax.fori_loop(0, groups, one, 0)

    def lower(r):
        at = pl.ds(pl.multiple_of(r * rows, rows), rows)
        partial[at, :] = lax.dot_general(
            down_w[at, :], act[...], (((1,), (1,)), ((), ())), preferred_element_type=jnp.float32
        ).astype(jnp.bfloat16)

    def fetch(w, j):
        source = firsts[w] if j == 0 else outs[w].at[j]
        return pltpu.make_async_copy(source, held_w[w], weight_sem.at[w])

    def keep(w):
        return pltpu.make_async_copy(held_w[w], outs[w].at[0], keep_sem.at[w])

    def level_at(d):
        return lax.rem(level // 2 + d // 2, 2) * 2 + lax.rem(level + d, 2)

    def across(j, d):
        goal = level_at(d) * 2 + 1 - side
        return pltpu.make_async_remote_copy(
            src_ref=partial.at[pl.ds(pl.multiple_of(goal * rows, rows), rows)],
            dst_ref=pair.at[j, d],
            send_sem=send_c.at[j, d],
            recv_sem=recv_c.at[j, d],
            device_id={"fs": mate},
            device_id_type=MESH,
        )

    def along_near(j, d):
        return pltpu.make_async_remote_copy(
            src_ref=to_near.at[j, d - 1],
            dst_ref=near.at[j, d - 1],
            send_sem=send_d.at[j, d - 1],
            recv_sem=recv_d.at[j, d - 1],
            device_id={"fs": level_at(1) * 2 + side},
            device_id_type=MESH,
        )

    def along_far(j):
        return pltpu.make_async_remote_copy(
            src_ref=to_far.at[j],
            dst_ref=far.at[j],
            send_sem=send_f.at[j],
            recv_sem=recv_f.at[j],
            device_id={"fs": level_at(3) * 2 + side},
            device_id_type=MESH,
        )

    def back(j, s):
        goal = lax.rem(me + s, groups)
        return pltpu.make_async_remote_copy(
            src_ref=total.at[j, :, pl.ds(pl.multiple_of(goal * capacity, capacity), capacity)],
            dst_ref=back_out.at[me, j],
            send_sem=send_e.at[j, s - 1],
            recv_sem=recv_e.at[j, s - 1],
            device_id={"tp": goal},
            device_id_type=MESH,
        )

    def kept(j):
        return pltpu.make_async_copy(
            total.at[j, :, pl.ds(pl.multiple_of(me * capacity, capacity), capacity)],
            back_out.at[me, j],
            last_sem.at[j],
        )

    def sum_into(j, d, target, others):
        base = (level_at(d) * 2 + side) * rows

        def add(i, carry):
            at = pl.ds(pl.multiple_of(i * strip, strip), strip)
            mine = pl.ds(pl.multiple_of(base + i * strip, strip), strip)
            value = partial[mine, :].astype(jnp.float32) + pair[j, d, at, :].astype(jnp.float32)
            for other in others:
                value = value + other[at, :].astype(jnp.float32)
            target[at, :] = value.astype(jnp.bfloat16)
            return carry

        lax.fori_loop(0, rows // strip, add, 0)

    def to_level(j, d):
        across(j, d).wait_recv()
        sum_into(j, d, to_near.at[j, d - 1], ())
        along_near(j, d).start()

    def cross_over(j):
        across(j, 3).wait_recv()
        along_near(j, 2).wait_recv()
        sum_into(j, 3, to_far.at[j], (near.at[j, 1],))
        along_far(j).start()

    def settle_sum(j):
        across(j, 0).wait_recv()
        along_near(j, 1).wait_recv()
        along_far(j).wait_recv()
        sum_into(j, 0, total.at[j], (near.at[j, 0], far.at[j]))
        for s in range(1, groups):
            back(j, s).start()
        kept(j).start()

    def after_0():
        for w in range(len(masters)):
            fetch(w, 0).start()
        pack(0)

    def after_1():
        for w in range(2):
            fetch(w, 0).wait()
            keep(w).start()
        hidden()

    def after_2():
        fetch(2, 0).wait()
        keep(2).start()

        def one(r, carry):
            lower(r)
            return carry

        lax.fori_loop(0, row_groups, one, 0)
        for d in range(stack):
            across(0, d).start()

    def after_3():
        to_level(0, 1)
        to_level(0, 2)

    def after_4():
        cross_over(0)

    tasks = {0: after_0, 1: after_1, 2: after_2, 3: after_3, 4: after_4}

    for n, (u, s) in enumerate(jobs):
        w, c = units[u]
        load(n).wait()
        slot = n % SLOTS

        def convert(i, carry):
            at = pl.ds(pl.multiple_of(i * strip, strip), strip)
            value = stage[slot, at, :]
            if w < 2:
                gain = gain_ref[pl.ds(pl.multiple_of(c * height + i * strip, strip), strip), :]
                value = value * gain
            cast[u, s, at, :] = value.astype(jnp.bfloat16)
            return carry

        lax.fori_loop(0, height // strip, convert, 0)
        if n + SLOTS < len(jobs):
            load(n + SLOTS).start()
        if s == 0:
            pass_on(u, 0)
            if u >= 1:
                forward(u - 1)
            if u in tasks:
                tasks[u]()
        else:
            first(u, s).start()
    forward(len(units) - 1)
    pack(1)
    settle_sum(0)
    for d in range(stack):
        across(0, d).wait_send()
    for w in range(2):
        keep(w).wait()
        for c in range(chunks):
            for source in range(row_groups):
                arrived(w * chunks + c, source)
        fetch(w, expert).start()
    for w in range(2):
        fetch(w, expert).wait()
    hidden()
    keep(2).wait()

    def piece(d, i):
        r = level_at(d) * 2 + lax.rem(side + 1 + i, 2)
        at = pl.ds(pl.multiple_of(r * rows, rows), rows)
        copy = pltpu.make_async_copy(outs[2].at[expert, at], down_w.at[at], raw_sem.at[i])
        return r, copy

    for d in range(stack):
        for i in range(2):
            r, copy = piece(d, i)
            for c in range(chunks):
                arrived(2 * chunks + c, r)
            copy.start()
        for i in range(2):
            piece(d, i)[1].wait()

        def one(i, carry):
            lower(level_at(d) * 2 + lax.rem(side + 1 + i, 2))
            return carry

        lax.fori_loop(0, 2, one, 0)
        across(1, d).start()
        if d >= 2:
            to_level(1, d - 1)
    cross_over(1)
    settle_sum(1)
    for d in range(stack):
        across(1, d).wait_send()
    for j in range(2):
        for d in (1, 2):
            along_near(j, d).wait_send()
        along_far(j).wait_send()
        kept(j).wait()
        for s in range(1, groups):
            back(j, s).wait()
    for u in range(len(units)):
        for s in range(groups):
            if s:
                first(u, s).wait_send()
            for b in range(blocks):
                goal, remote, local = second(u, s, b)

                @pl.when(goal != row)
                def _():
                    remote().wait_send()


def serve(gain, gate, up, down, everything, spots, firsts, expert, collective):
    groups = lax.axis_size("tp")
    row_groups = lax.axis_size("fs")
    experts, rows, columns = gate.shape
    blocks = row_groups // groups
    width = columns // blocks
    model_width = rows * row_groups
    tokens = spots.shape[2]
    capacity = tokens // 2
    slots = groups * capacity
    chunks = 2
    units = 3 * chunks
    height = rows // chunks
    stack = row_groups // 2
    out = jax.ShapeDtypeStruct((experts // groups, model_width, width), jnp.bfloat16)
    hbm = pl.BlockSpec(memory_space=pl.ANY)
    vmem = pl.BlockSpec(memory_space=pltpu.VMEM)
    sent = 3 * rows * columns * 2 * groups
    weight = pltpu.VMEM((model_width, width), jnp.bfloat16)
    dma = lambda *shape: pltpu.SemaphoreType.DMA(shape)
    return pl.pallas_call(
        functools.partial(serve_kernel, groups, row_groups, expert, chunks),
        out_shape=(
            out, out, out,
            jax.ShapeDtypeStruct((groups, 2, rows, capacity), jnp.bfloat16),
        ),
        in_specs=[vmem, hbm, hbm, hbm, hbm, vmem, hbm, hbm, hbm],
        out_specs=(hbm,) * 4,
        scratch_shapes=[
            pltpu.VMEM((SLOTS, height, columns), jnp.float32),
            pltpu.VMEM((units, groups, height, columns), jnp.bfloat16),
            pltpu.VMEM((units, groups - 1, height, columns), jnp.bfloat16),
            pltpu.VMEM((tokens, model_width), jnp.bfloat16),
            pltpu.VMEM((slots, model_width), jnp.bfloat16),
            weight, weight, weight,
            pltpu.VMEM((slots, width), jnp.bfloat16),
            pltpu.VMEM((model_width, slots), jnp.bfloat16),
            pltpu.VMEM((2, stack, rows, slots), jnp.bfloat16),
            pltpu.VMEM((2, 2, rows, slots), jnp.bfloat16),
            pltpu.VMEM((2, 2, rows, slots), jnp.bfloat16),
            pltpu.VMEM((2, rows, slots), jnp.bfloat16),
            pltpu.VMEM((2, rows, slots), jnp.bfloat16),
            pltpu.VMEM((2, rows, slots), jnp.bfloat16),
            dma(SLOTS), dma(units, groups - 1), dma(units, groups - 1),
            dma(units, row_groups), dma(units, row_groups),
            dma(row_groups), dma(3), dma(3),
            dma(2, stack), dma(2, stack), dma(2, 2), dma(2, 2), dma(2), dma(2),
            dma(2, groups - 1), dma(2, groups - 1), dma(2),
        ],
        compiler_params=pltpu.CompilerParams(
            collective_id=collective, has_side_effects=True, vmem_limit_bytes=62 * 1024 * 1024
        ),
        cost_estimate=pl.CostEstimate(
            flops=12 * slots * model_width * width, bytes_accessed=32 * sent, transcendentals=0
        ),
    )(gain, gate, up, down, everything, spots, *firsts)


def fused_device(
    hidden_states, norm_gain, gate_master, up_master, down_master, expert_ids, route_logits
):
    groups = lax.axis_size("tp")
    experts = gate_master.shape[0]
    local_count = experts // groups
    tokens, pieces = hidden_states.shape
    capacity = tokens // 2
    gain = norm_gain[:, None]
    earlier = (jnp.arange(tokens)[:, None] > jnp.arange(tokens)[None, :]).astype(jnp.bfloat16)
    weights = jax.nn.softmax(route_logits, axis=1)
    named = expert_ids[:, :, None] == jnp.arange(experts, dtype=jnp.int32)[None, None, :]
    chosen = jnp.any(named, axis=1).astype(jnp.bfloat16)
    before = jnp.dot(earlier, chosen, preferred_element_type=jnp.float32)
    position = jnp.sum(jnp.where(named, before[:, None, :], 0.0), axis=2).astype(jnp.int32)
    slot_ids = (expert_ids * capacity + position).reshape(-1)

    spots = jnp.where(chosen > 0, before, -1.0).T.reshape(groups, local_count, tokens)
    *firsts, everything, spots = exchange(
        gain, gate_master, up_master, down_master, hidden_states, spots, 0, 1
    )
    gate, up, down, ordered = serve(
        gain, gate_master, up_master, down_master, everything, spots, firsts, 1, 2
    )
    flat_out = jnp.moveaxis(ordered, 2, 0).reshape(pieces, experts * capacity)
    picked = flat_out.at[:, slot_ids].get(mode="promise_in_bounds")
    picked = picked.reshape(pieces, tokens, 2).astype(jnp.float32)
    combined = jnp.sum(picked * weights[None, :, :], axis=2)
    return gate, up, down, jnp.transpose(combined).astype(jnp.bfloat16)


def arrange(weights, groups, row_groups):
    experts, rows, columns = weights.shape
    blocks = row_groups // groups
    split = weights.reshape(experts // groups, groups, rows, blocks, columns // blocks)
    split = split.reshape(groups, experts // groups, rows, blocks, columns // blocks)
    return jnp.transpose(split, (0, 3, 1, 2, 4))


def regroup(moved, row_groups):
    return moved.reshape((row_groups,) + moved.shape[2:])


def settle(arrived):
    return arrived.reshape(arrived.shape[1], arrived.shape[2], arrived.shape[3])


def per_device(
    hidden_states, norm_gain, gate_master, up_master, down_master, expert_ids, route_logits
):
    groups = lax.axis_size("tp")
    row_groups = lax.axis_size("fs")
    whole_tiles = gate_master.shape[2] // (row_groups // groups) % 128 == 0
    lined = groups == 4 and row_groups == 8
    if whole_tiles and lined and gate_master.shape[0] == 2 * groups:
        return fused_device(
            hidden_states, norm_gain, gate_master, up_master, down_master, expert_ids, route_logits
        )
    experts = gate_master.shape[0]
    local_count = experts // groups
    tokens = hidden_states.shape[0]
    pieces = hidden_states.shape[1]
    model_width = pieces * row_groups
    capacity = tokens // 2
    scaled = norm_gain[None, :, None]
    gate_cast = arrange((scaled * gate_master).astype(jnp.bfloat16), groups, row_groups)
    up_cast = arrange((scaled * up_master).astype(jnp.bfloat16), groups, row_groups)
    down_cast = arrange(down_master.astype(jnp.bfloat16), groups, row_groups)
    sectioned = (
        lax.all_to_all(gate_cast, "tp", split_axis=0, concat_axis=0, tiled=True),
        lax.all_to_all(up_cast, "tp", split_axis=0, concat_axis=0, tiled=True),
        lax.all_to_all(down_cast, "tp", split_axis=0, concat_axis=0, tiled=True),
    )
    landed = (
        lax.all_to_all(
            regroup(sectioned[0], row_groups), "fs", split_axis=0, concat_axis=2, tiled=True
        ),
        lax.all_to_all(
            regroup(sectioned[1], row_groups), "fs", split_axis=0, concat_axis=2, tiled=True
        ),
        lax.all_to_all(
            regroup(sectioned[2], row_groups), "fs", split_axis=0, concat_axis=2, tiled=True
        ),
    )
    gate_serve, up_serve, down_serve = (settle(landed[0]), settle(landed[1]), settle(landed[2]))
    values = hidden_states.astype(jnp.float32)
    squares = lax.psum(jnp.sum(values * values, axis=1), "fs")
    normed = (values * lax.rsqrt(squares / model_width + EPSILON)[:, None]).astype(jnp.bfloat16)
    weights = jax.nn.softmax(route_logits, axis=1)
    chosen = (expert_ids[:, :, None] == jnp.arange(experts, dtype=jnp.int32)[None, None, :]).astype(
        jnp.int32
    )
    chosen = chosen.reshape(tokens * 2, experts)
    before = jnp.cumsum(chosen, axis=0) - chosen
    position = jnp.sum(before * chosen, axis=1)
    slot_ids = expert_ids.reshape(-1) * capacity + position
    slot_table = (
        slot_ids[None, :] == jnp.arange(experts * capacity, dtype=jnp.int32)[:, None]
    ).astype(jnp.bfloat16)
    dispatch = jnp.sum(slot_table.reshape(experts * capacity, tokens, 2), axis=2)
    whole_rows = lax.all_gather(normed, "fs", axis=1, tiled=True)
    packed = jnp.dot(dispatch, whole_rows, preferred_element_type=jnp.float32).astype(jnp.bfloat16)
    arrived = lax.all_to_all(
        packed.reshape(groups, local_count * capacity, model_width),
        "tp",
        split_axis=0,
        concat_axis=0,
        tiled=True,
    )
    arranged = arrived.reshape(groups, local_count, capacity, model_width)
    activations = []
    for expert_index in range(local_count):
        expert_rows = arranged[:, expert_index].reshape(groups * capacity, model_width)
        gate_pre = jnp.dot(
            expert_rows, gate_serve[expert_index], preferred_element_type=jnp.float32
        )
        up_pre = jnp.dot(expert_rows, up_serve[expert_index], preferred_element_type=jnp.float32)
        activations.append((jax.nn.silu(gate_pre) * up_pre).astype(jnp.bfloat16))
    stacked = jnp.stack(activations)
    summed = lax.psum_scatter(
        jnp.einsum("jdh,jsh->djs", down_serve, stacked, preferred_element_type=jnp.float32).astype(
            jnp.bfloat16
        ),
        "fs",
        scatter_dimension=0,
        tiled=True,
    )
    results = summed.reshape(pieces, local_count, groups, capacity)
    returned = lax.all_to_all(results, "tp", split_axis=2, concat_axis=1, tiled=True)
    flat_out = returned.reshape(pieces, experts * capacity)
    picked = jnp.take(flat_out, slot_ids, axis=1).reshape(pieces, tokens, 2).astype(jnp.float32)
    combined = jnp.sum(picked * weights[None, :, :], axis=2)
    return (gate_serve, up_serve, down_serve, jnp.transpose(combined).astype(jnp.bfloat16))


def solution(mesh):
    in_specs = (
        P("tp", "fs"),
        P("fs"),
        P(None, "fs", "tp"),
        P(None, "fs", "tp"),
        P(None, "fs", "tp"),
        P("tp", None),
        P("tp", None),
    )
    out_specs = (P("tp", None, "fs"), P("tp", None, "fs"), P("tp", None, "fs"), P("tp", "fs"))
    return jax.shard_map(
        per_device, mesh=mesh, in_specs=in_specs, out_specs=out_specs, check_vma=False
    )
```

```python
import functools

import jax
import jax.numpy as jnp
from jax import lax
from jax.experimental import pallas as pl
from jax.experimental.pallas import tpu as pltpu
from jax.sharding import PartitionSpec as P

EPSILON = 1e-06
SLOTS = 4
MESH = pl.DeviceIdType.MESH


def exchange_kernel(
    groups, row_groups, expert, chunks, gain_ref, gate_ref, up_ref, down_ref, own_ref, spot_ref,
    gate_out, up_out, down_out, all_out, spot_out, stage, cast, landed, load_sem,
    send_a, recv_a, send_b, recv_b, send_z, recv_z, send_y, recv_y, send_t, recv_t,
    send_s, recv_s, own_sem,
):
    me = lax.axis_index("tp")
    row = lax.axis_index("fs")
    blocks = row_groups // groups
    masters = (gate_ref, up_ref, down_ref)
    outs = (gate_out, up_out, down_out)
    local_count = gate_ref.shape[0] // groups
    rows, columns = gate_ref.shape[1:]
    height = rows // chunks
    width = columns // blocks

    barrier = pltpu.get_barrier_semaphore()
    for step in range(1, groups):
        pl.semaphore_signal(
            barrier, inc=1, device_id={"tp": lax.rem(me + step, groups)}, device_id_type=MESH
        )
    for step in range(1, row_groups):
        pl.semaphore_signal(
            barrier, inc=1, device_id={"fs": lax.rem(row + step, row_groups)}, device_id_type=MESH
        )
    rest = [s for s in range(1, groups) if s != groups // 2]
    order = [groups // 2] + rest + [0]
    opening = [groups // 2, 0] + rest
    units = [(w, c) for w in range(len(masters)) for c in range(chunks)]
    jobs = [(u, s) for u in range(len(units)) for s in (order if u else opening)]

    def load(n):
        u, s = jobs[n]
        w, c = units[u]
        number = lax.rem(me + s, groups) * local_count + expert
        return pltpu.make_async_copy(
            masters[w].at[number, pl.ds(c * height, height)],
            stage.at[n % SLOTS],
            load_sem.at[n % SLOTS],
        )

    for n in range(SLOTS):
        load(n).start()
    pl.semaphore_wait(barrier, groups - 1 + row_groups - 1)

    def first(u, s):
        return pltpu.make_async_remote_copy(
            src_ref=cast.at[u, s],
            dst_ref=landed.at[u, s - 1],
            send_sem=send_a.at[u, s - 1],
            recv_sem=recv_a.at[u, s - 1],
            device_id={"tp": lax.rem(me + s, groups)},
            device_id_type=MESH,
        )

    def place(u, source):
        w, c = units[u]
        start = pl.multiple_of(source * rows + c * height, height)
        return outs[w].at[pl.ds(start, height)]

    def second(u, s, b):
        held = cast.at[u, 0] if s == 0 else landed.at[u, s - 1]
        goal = lax.rem(me + groups - s, groups) * blocks + b
        piece = held.at[:, pl.ds(b * width, width)]
        remote = lambda: pltpu.make_async_remote_copy(
            src_ref=piece,
            dst_ref=place(u, row),
            send_sem=send_b.at[u, s * blocks + b],
            recv_sem=recv_b.at[u, row],
            device_id={"fs": goal},
            device_id_type=MESH,
        )
        local = lambda: pltpu.make_async_copy(piece, place(u, row), recv_b.at[u, row])
        return goal, remote, local

    def pass_on(u, s):
        for b in range(blocks):
            goal, remote, local = second(u, s, b)

            @pl.when(goal != row)
            def _():
                remote().start()

            @pl.when(goal == row)
            def _():
                local().start()

    def forward(u):
        for s in sorted(range(1, groups), key=lambda s: s == groups // 2):
            first(u, s).wait_recv()
            pass_on(u, s)

    side = lax.rem(row, 2)
    mate = row + 1 - 2 * side
    stack = row_groups // 2
    level = row // 2

    def block(k, y):
        which = side if y == 0 else 1 - side
        return lax.rem(level + stack - k, stack) * 2 + which

    def up_z(k):
        return pltpu.make_async_remote_copy(
            src_ref=own_ref,
            dst_ref=all_out.at[row, me],
            send_sem=send_z.at[k - 1],
            recv_sem=recv_z.at[k - 1],
            device_id={"fs": lax.rem(level + k, stack) * 2 + side},
            device_id_type=MESH,
        )

    def over_y(k):
        place = all_out.at[block(k, 0), me]
        return pltpu.make_async_remote_copy(
            src_ref=own_ref if k == 0 else place,
            dst_ref=place,
            send_sem=send_y.at[k],
            recv_sem=recv_y.at[k],
            device_id={"fs": mate},
            device_id_type=MESH,
        )

    def over_tp(k, y, s):
        place = all_out.at[block(k, y), me]
        return pltpu.make_async_remote_copy(
            src_ref=own_ref if k == 0 and y == 0 else place,
            dst_ref=place,
            send_sem=send_t.at[y * stack + k, s - 1],
            recv_sem=recv_t.at[y * stack + k, s - 1],
            device_id={"tp": lax.rem(me + s, groups)},
            device_id_type=MESH,
        )

    def spots_to(s):
        goal = lax.rem(me + s, groups)
        return pltpu.make_async_remote_copy(
            src_ref=spot_ref.at[goal],
            dst_ref=spot_out.at[me],
            send_sem=send_s.at[s - 1],
            recv_sem=recv_s.at[s - 1],
            device_id={"tp": goal},
            device_id_type=MESH,
        )

    own_kept = pltpu.make_async_copy(own_ref, all_out.at[row, me], own_sem.at[0])
    spot_kept = pltpu.make_async_copy(spot_ref.at[me], spot_out.at[me], own_sem.at[1])
    own_kept.start()
    spot_kept.start()
    for k in range(1, stack):
        up_z(k).start()
    over_y(0).start()
    for s in range(1, groups):
        spots_to(s).start()

    def near_blocks():
        for k in range(stack):
            if k:
                up_z(k).wait_recv()
                over_y(k).start()
            for s in range(1, groups):
                over_tp(k, 0, s).start()

    def far_blocks():
        for k in range(stack):
            over_y(k).wait_recv()
            for s in range(1, groups):
                over_tp(k, 1, s).start()

    tasks = {1: near_blocks, 3: far_blocks}
    strip = 16
    for n, (u, s) in enumerate(jobs):
        w, c = units[u]
        load(n).wait()
        slot = n % SLOTS

        def convert(i, carry):
            at = pl.ds(pl.multiple_of(i * strip, strip), strip)
            value = stage[slot, at, :]
            if w < 2:
                gain = gain_ref[pl.ds(pl.multiple_of(c * height + i * strip, strip), strip), :]
                value = value * gain
            cast[u, s, at, :] = value.astype(jnp.bfloat16)
            return carry

        lax.fori_loop(0, height // strip, convert, 0)
        if n + SLOTS < len(jobs):
            load(n + SLOTS).start()
        if s == 0:
            pass_on(u, 0)
        else:
            first(u, s).start()
        if n + 1 == len(jobs) or jobs[n + 1][0] != u:
            if u >= 1:
                forward(u - 1)
            if u in tasks:
                tasks[u]()
    forward(len(units) - 1)
    own_kept.wait()
    spot_kept.wait()
    for k in range(stack):
        if k:
            up_z(k).wait_send()
        over_y(k).wait_send()
        for s in range(1, groups):
            for y in range(2):
                over_tp(k, y, s).wait()
    for s in range(1, groups):
        spots_to(s).wait()
    for u in range(len(units)):
        for s in range(groups):
            if s:
                first(u, s).wait_send()
            for b in range(blocks):
                goal, remote, local = second(u, s, b)

                @pl.when(goal != row)
                def _():
                    remote().wait_send()
        for source in range(row_groups):
            pltpu.make_async_copy(
                cast.at[u, 0, :, pl.ds(0, width)], place(u, source), recv_b.at[u, source]
            ).wait()


def exchange(gain, gate, up, down, hidden, spots, expert, collective):
    groups = lax.axis_size("tp")
    row_groups = lax.axis_size("fs")
    experts, rows, columns = gate.shape
    blocks = row_groups // groups
    width = columns // blocks
    chunks = 2
    units = 3 * chunks
    height = rows // chunks
    out = jax.ShapeDtypeStruct((rows * row_groups, width), jnp.bfloat16)
    hbm = pl.BlockSpec(memory_space=pl.ANY)
    stack = row_groups // 2
    vmem = pl.BlockSpec(memory_space=pltpu.VMEM)
    sent = 3 * rows * columns * 2 * groups
    dma = lambda *shape: pltpu.SemaphoreType.DMA(shape)
    return pl.pallas_call(
        functools.partial(exchange_kernel, groups, row_groups, expert, chunks),
        out_shape=(
            out, out, out,
            jax.ShapeDtypeStruct((row_groups, groups) + hidden.shape, hidden.dtype),
            jax.ShapeDtypeStruct(spots.shape, spots.dtype),
        ),
        in_specs=[vmem, hbm, hbm, hbm, vmem, vmem],
        out_specs=(hbm,) * 5,
        scratch_shapes=[
            pltpu.VMEM((SLOTS, height, columns), jnp.float32),
            pltpu.VMEM((units, groups, height, columns), jnp.bfloat16),
            pltpu.VMEM((units, groups - 1, height, columns), jnp.bfloat16),
            dma(SLOTS), dma(units, groups - 1), dma(units, groups - 1),
            dma(units, row_groups), dma(units, row_groups),
            dma(stack - 1), dma(stack - 1), dma(stack), dma(stack),
            dma(2 * stack, groups - 1), dma(2 * stack, groups - 1),
            dma(groups - 1), dma(groups - 1), dma(2),
        ],
        compiler_params=pltpu.CompilerParams(
            collective_id=collective, has_side_effects=True, vmem_limit_bytes=62 * 1024 * 1024
        ),
        cost_estimate=pl.CostEstimate(
            flops=rows * columns, bytes_accessed=32 * sent, transcendentals=0
        ),
    )(gain, gate, up, down, hidden, spots)


def serve_kernel(
    groups, row_groups, expert, chunks, gain_ref, gate_ref, up_ref, down_ref, all_ref, spot_ref,
    gate_first, up_first, down_first,
    gate_out, up_out, down_out, back_out,
    stage, cast, landed, raw, rows_in, gate_w, up_w, down_w, act, partial,
    pair, to_near, near, to_far, far, total,
    load_sem, send_a, recv_a, send_b, recv_b, raw_sem, weight_sem, keep_sem,
    send_c, recv_c, send_d, recv_d, send_f, recv_f, send_e, recv_e, last_sem,
):
    me = lax.axis_index("tp")
    row = lax.axis_index("fs")
    blocks = row_groups // groups
    masters = (gate_ref, up_ref, down_ref)
    outs = (gate_out, up_out, down_out)
    firsts = (gate_first, up_first, down_first)
    held_w = (gate_w, up_w, down_w)
    local_count = gate_ref.shape[0] // groups
    rows, columns = gate_ref.shape[1:]
    height = rows // chunks
    width = columns // blocks
    tokens, model_width = raw.shape
    capacity = tokens // 2
    side = lax.rem(row, 2)
    mate = row + 1 - 2 * side
    stack = row_groups // 2
    level = row // 2
    strip = 16

    barrier = pltpu.get_barrier_semaphore()
    for step in range(1, groups):
        pl.semaphore_signal(
            barrier, inc=1, device_id={"tp": lax.rem(me + step, groups)}, device_id_type=MESH
        )
    for step in range(1, row_groups):
        pl.semaphore_signal(
            barrier, inc=1, device_id={"fs": lax.rem(row + step, row_groups)}, device_id_type=MESH
        )
    rest = [s for s in range(1, groups) if s != groups // 2]
    order = [groups // 2] + rest + [0]
    opening = [groups // 2, 0] + rest
    units = [(w, c) for w in range(len(masters)) for c in range(chunks)]
    jobs = [(u, s) for u in range(len(units)) for s in (order if u else opening)]

    def load(n):
        u, s = jobs[n]
        w, c = units[u]
        number = lax.rem(me + s, groups) * local_count + expert
        return pltpu.make_async_copy(
            masters[w].at[number, pl.ds(c * height, height)],
            stage.at[n % SLOTS],
            load_sem.at[n % SLOTS],
        )

    for n in range(SLOTS):
        load(n).start()
    pl.semaphore_wait(barrier, groups - 1 + row_groups - 1)

    def first(u, s):
        return pltpu.make_async_remote_copy(
            src_ref=cast.at[u, s],
            dst_ref=landed.at[u, s - 1],
            send_sem=send_a.at[u, s - 1],
            recv_sem=recv_a.at[u, s - 1],
            device_id={"tp": lax.rem(me + s, groups)},
            device_id_type=MESH,
        )

    def place(u, source):
        w, c = units[u]
        start = pl.multiple_of(source * rows + c * height, height)
        return outs[w].at[expert, pl.ds(start, height)]

    def second(u, s, b):
        held = cast.at[u, 0] if s == 0 else landed.at[u, s - 1]
        goal = lax.rem(me + groups - s, groups) * blocks + b
        piece = held.at[:, pl.ds(b * width, width)]
        remote = lambda: pltpu.make_async_remote_copy(
            src_ref=piece,
            dst_ref=place(u, row),
            send_sem=send_b.at[u, s * blocks + b],
            recv_sem=recv_b.at[u, row],
            device_id={"fs": goal},
            device_id_type=MESH,
        )
        local = lambda: pltpu.make_async_copy(piece, place(u, row), recv_b.at[u, row])
        return goal, remote, local

    def pass_on(u, s):
        for b in range(blocks):
            goal, remote, local = second(u, s, b)

            @pl.when(goal != row)
            def _():
                remote().start()

            @pl.when(goal == row)
            def _():
                local().start()

    def forward(u):
        for s in sorted(range(1, groups), key=lambda s: s == groups // 2):
            first(u, s).wait_recv()
            pass_on(u, s)

    def arrived(u, source):
        pltpu.make_async_copy(
            cast.at[u, 0, :, pl.ds(0, width)], place(u, source), recv_b.at[u, source]
        ).wait()

    def pack(j):
        def one(g, carry):
            copies = [
                pltpu.make_async_copy(
                    all_ref.at[f, g],
                    raw.at[:, pl.ds(f * (model_width // row_groups), model_width // row_groups)],
                    raw_sem.at[f],
                )
                for f in range(row_groups)
            ]
            for copy in copies:
                copy.start()
            for copy in copies:
                copy.wait()
            spot = spot_ref[g, pl.ds(j, 1), :]
            slot = lax.broadcasted_iota(jnp.int32, (capacity, tokens), 0).astype(jnp.float32)
            table = jnp.where(slot == spot, 1.0, 0.0).astype(jnp.bfloat16)
            packed = jnp.dot(table, raw[...], preferred_element_type=jnp.float32)
            mean = jnp.mean(packed * packed, axis=1, keepdims=True)
            at = pl.ds(pl.multiple_of(g * capacity, capacity), capacity)
            rows_in[at, :] = (packed * lax.rsqrt(mean + EPSILON)).astype(jnp.bfloat16)
            return carry

        lax.fori_loop(0, groups, one, 0)

    def hidden():
        def one(t, carry):
            at = pl.ds(pl.multiple_of(t * capacity, capacity), capacity)
            value = rows_in[at, :]
            gate_pre = jnp.dot(value, gate_w[...], preferred_element_type=jnp.float32)
            up_pre = jnp.dot(value, up_w[...], preferred_element_type=jnp.float32)
            act[at, :] = (gate_pre / (1.0 + jnp.exp(-gate_pre)) * up_pre).astype(jnp.bfloat16)
            return carry

        lax.fori_loop(0, groups, one, 0)

    def lower(start, size):
        at = pl.ds(pl.multiple_of(start, size), size)
        partial[at, :] = lax.dot_general(
            down_w[at, :], act[...], (((1,), (1,)), ((), ())), preferred_element_type=jnp.float32
        ).astype(jnp.bfloat16)

    def fetch(w, j):
        source = firsts[w] if j == 0 else outs[w].at[j]
        return pltpu.make_async_copy(source, held_w[w], weight_sem.at[w])

    def keep(w):
        return pltpu.make_async_copy(held_w[w], outs[w].at[0], keep_sem.at[w])

    def level_at(d):
        return lax.rem(level // 2 + d // 2, 2) * 2 + lax.rem(level + d, 2)

    def span(c):
        return pl.ds(c * height, height)

    def across(j, d, c):
        start = (level_at(d) * 2 + 1 - side) * rows + c * height
        return pltpu.make_async_remote_copy(
            src_ref=partial.at[pl.ds(pl.multiple_of(start, height), height)],
            dst_ref=pair.at[j, d, span(c)],
            send_sem=send_c.at[j, d, c],
            recv_sem=recv_c.at[j, d, c],
            device_id={"fs": mate},
            device_id_type=MESH,
        )

    def along_near(j, d, c):
        return pltpu.make_async_remote_copy(
            src_ref=to_near.at[j, d - 1, span(c)],
            dst_ref=near.at[j, d - 1, span(c)],
            send_sem=send_d.at[j, d - 1, c],
            recv_sem=recv_d.at[j, d - 1, c],
            device_id={"fs": level_at(1) * 2 + side},
            device_id_type=MESH,
        )

    def along_far(j, c):
        return pltpu.make_async_remote_copy(
            src_ref=to_far.at[j, span(c)],
            dst_ref=far.at[j, span(c)],
            send_sem=send_f.at[j, c],
            recv_sem=recv_f.at[j, c],
            device_id={"fs": level_at(3) * 2 + side},
            device_id_type=MESH,
        )

    def back(j, s, c):
        goal = lax.rem(me + s, groups)
        columns = pl.ds(pl.multiple_of(goal * capacity, capacity), capacity)
        return pltpu.make_async_remote_copy(
            src_ref=total.at[j, span(c), columns],
            dst_ref=back_out.at[me, j, span(c)],
            send_sem=send_e.at[j, s - 1, c],
            recv_sem=recv_e.at[j, s - 1, c],
            device_id={"tp": goal},
            device_id_type=MESH,
        )

    def kept(j, c):
        columns = pl.ds(pl.multiple_of(me * capacity, capacity), capacity)
        return pltpu.make_async_copy(
            total.at[j, span(c), columns], back_out.at[me, j, span(c)], last_sem.at[j, c]
        )

    def sum_into(j, d, c, target, others):
        base = (level_at(d) * 2 + side) * rows

        def add(i, carry):
            at = pl.ds(pl.multiple_of(c * height + i * strip, strip), strip)
            mine = pl.ds(pl.multiple_of(base + c * height + i * strip, strip), strip)
            value = partial[mine, :].astype(jnp.float32) + pair[j, d, at, :].astype(jnp.float32)
            for other in others:
                value = value + other[at, :].astype(jnp.float32)
            target[at, :] = value.astype(jnp.bfloat16)
            return carry

        lax.fori_loop(0, height // strip, add, 0)

    def to_level(j, d, c):
        across(j, d, c).wait_recv()
        sum_into(j, d, c, to_near.at[j, d - 1], ())
        along_near(j, d, c).start()

    def cross_over(j, c):
        across(j, 3, c).wait_recv()
        along_near(j, 2, c).wait_recv()
        sum_into(j, 3, c, to_far.at[j], (near.at[j, 1],))
        along_far(j, c).start()

    def settle_sum(j, c):
        across(j, 0, c).wait_recv()
        along_near(j, 1, c).wait_recv()
        along_far(j, c).wait_recv()
        sum_into(j, 0, c, total.at[j], (near.at[j, 0], far.at[j]))
        for s in range(1, groups):
            back(j, s, c).start()
        kept(j, c).start()

    def after_0():
        for w in range(len(masters)):
            fetch(w, 0).start()
        pack(0)

    def after_1():
        for w in range(2):
            fetch(w, 0).wait()
            keep(w).start()
        hidden()

    def after_2():
        fetch(2, 0).wait()
        keep(2).start()

        def one(r, carry):
            lower(r * rows, rows)
            return carry

        lax.fori_loop(0, row_groups, one, 0)
        for c in range(chunks):
            for d in range(stack):
                across(0, d, c).start()

    def after_3():
        for c in range(chunks):
            to_level(0, 2, c)
            to_level(0, 1, c)

    def after_4():
        for c in range(chunks):
            cross_over(0, c)

    tasks = {0: after_0, 1: after_1, 2: after_2, 3: after_3, 4: after_4}

    for n, (u, s) in enumerate(jobs):
        w, c = units[u]
        load(n).wait()
        slot = n % SLOTS

        def convert(i, carry):
            at = pl.ds(pl.multiple_of(i * strip, strip), strip)
            value = stage[slot, at, :]
            if w < 2:
                gain = gain_ref[pl.ds(pl.multiple_of(c * height + i * strip, strip), strip), :]
                value = value * gain
            cast[u, s, at, :] = value.astype(jnp.bfloat16)
            return carry

        lax.fori_loop(0, height // strip, convert, 0)
        if n + SLOTS < len(jobs):
            load(n + SLOTS).start()
        if s == 0:
            pass_on(u, 0)
        else:
            first(u, s).start()
        if n + 1 == len(jobs) or jobs[n + 1][0] != u:
            if u >= 1:
                forward(u - 1)
            if u in tasks:
                tasks[u]()
    forward(len(units) - 1)
    pack(1)
    for c in range(chunks):
        settle_sum(0, c)
        for d in range(stack):
            across(0, d, c).wait_send()
    for w in range(2):
        keep(w).wait()
        for c in range(chunks):
            for source in range(row_groups):
                arrived(w * chunks + c, source)
        fetch(w, expert).start()
    for w in range(2):
        fetch(w, expert).wait()
    hidden()
    keep(2).wait()

    def piece(d, i, c):
        source = level_at(d) * 2 + lax.rem(side + 1 + i, 2)
        at = pl.ds(pl.multiple_of(source * rows + c * height, height), height)
        copy = pltpu.make_async_copy(outs[2].at[expert, at], down_w.at[at], raw_sem.at[i])
        return source, copy

    def level_product(d, c):
        for i in range(2):
            source, copy = piece(d, i, c)
            arrived(2 * chunks + c, source)
            copy.start()
        for i in range(2):
            piece(d, i, c)[1].wait()

        def one(i, carry):
            lower((level_at(d) * 2 + lax.rem(side + 1 + i, 2)) * rows + c * height, height)
            return carry

        lax.fori_loop(0, 2, one, 0)
        across(1, d, c).start()

    for c in range(chunks):
        for d in range(stack):
            if c and d == 2:
                to_level(1, 2, c - 1)
                to_level(1, 1, c - 1)
            level_product(d, c)
        if c:
            cross_over(1, c - 1)
    to_level(1, 2, chunks - 1)
    to_level(1, 1, chunks - 1)
    cross_over(1, chunks - 1)
    for c in range(chunks):
        settle_sum(1, c)
    for c in range(chunks):
        for d in range(stack):
            across(1, d, c).wait_send()
        for j in range(2):
            for d in (1, 2):
                along_near(j, d, c).wait_send()
            along_far(j, c).wait_send()
            kept(j, c).wait()
            for s in range(1, groups):
                back(j, s, c).wait()
    for u in range(len(units)):
        for s in range(groups):
            if s:
                first(u, s).wait_send()
            for b in range(blocks):
                goal, remote, local = second(u, s, b)

                @pl.when(goal != row)
                def _():
                    remote().wait_send()


def serve(gain, gate, up, down, everything, spots, firsts, expert, collective):
    groups = lax.axis_size("tp")
    row_groups = lax.axis_size("fs")
    experts, rows, columns = gate.shape
    blocks = row_groups // groups
    width = columns // blocks
    model_width = rows * row_groups
    tokens = spots.shape[2]
    capacity = tokens // 2
    slots = groups * capacity
    chunks = 2
    units = 3 * chunks
    height = rows // chunks
    stack = row_groups // 2
    out = jax.ShapeDtypeStruct((experts // groups, model_width, width), jnp.bfloat16)
    hbm = pl.BlockSpec(memory_space=pl.ANY)
    vmem = pl.BlockSpec(memory_space=pltpu.VMEM)
    sent = 3 * rows * columns * 2 * groups
    weight = pltpu.VMEM((model_width, width), jnp.bfloat16)
    dma = lambda *shape: pltpu.SemaphoreType.DMA(shape)
    return pl.pallas_call(
        functools.partial(serve_kernel, groups, row_groups, expert, chunks),
        out_shape=(
            out, out, out,
            jax.ShapeDtypeStruct((groups, 2, rows, capacity), jnp.bfloat16),
        ),
        in_specs=[vmem, hbm, hbm, hbm, hbm, vmem, hbm, hbm, hbm],
        out_specs=(hbm,) * 4,
        scratch_shapes=[
            pltpu.VMEM((SLOTS, height, columns), jnp.float32),
            pltpu.VMEM((units, groups, height, columns), jnp.bfloat16),
            pltpu.VMEM((units, groups - 1, height, columns), jnp.bfloat16),
            pltpu.VMEM((tokens, model_width), jnp.bfloat16),
            pltpu.VMEM((slots, model_width), jnp.bfloat16),
            weight, weight, weight,
            pltpu.VMEM((slots, width), jnp.bfloat16),
            pltpu.VMEM((model_width, slots), jnp.bfloat16),
            pltpu.VMEM((2, stack, rows, slots), jnp.bfloat16),
            pltpu.VMEM((2, 2, rows, slots), jnp.bfloat16),
            pltpu.VMEM((2, 2, rows, slots), jnp.bfloat16),
            pltpu.VMEM((2, rows, slots), jnp.bfloat16),
            pltpu.VMEM((2, rows, slots), jnp.bfloat16),
            pltpu.VMEM((2, rows, slots), jnp.bfloat16),
            dma(SLOTS), dma(units, groups - 1), dma(units, groups - 1),
            dma(units, row_groups), dma(units, row_groups),
            dma(row_groups), dma(3), dma(3),
            dma(2, stack, chunks), dma(2, stack, chunks),
            dma(2, 2, chunks), dma(2, 2, chunks), dma(2, chunks), dma(2, chunks),
            dma(2, groups - 1, chunks), dma(2, groups - 1, chunks), dma(2, chunks),
        ],
        compiler_params=pltpu.CompilerParams(
            collective_id=collective, has_side_effects=True, vmem_limit_bytes=62 * 1024 * 1024
        ),
        cost_estimate=pl.CostEstimate(
            flops=12 * slots * model_width * width, bytes_accessed=32 * sent, transcendentals=0
        ),
    )(gain, gate, up, down, everything, spots, *firsts)


def finish_kernel(
    parts, gate_ref, up_ref, down_ref, back_ref, slot_ref, logit_ref,
    gate_out, up_out, down_out, out_ref, held, load_sem, store_sem,
):
    sources = (gate_ref, up_ref, down_ref)
    goals = (gate_out, up_out, down_out)
    local_count, height, width = gate_ref.shape
    part = height // parts
    pieces = [
        (w, j, pl.ds(p * part, part))
        for w in range(3) for j in range(local_count) for p in range(parts)
    ]

    def load(n):
        w, j, at = pieces[n]
        return pltpu.make_async_copy(sources[w].at[j, at], held.at[n], load_sem.at[n])

    def store(n):
        w, j, at = pieces[n]
        return pltpu.make_async_copy(held.at[n], goals[w].at[j, at], store_sem.at[n])

    for n in range(len(pieces)):
        load(n).start()
    tokens, features = out_ref.shape
    groups, count, _, capacity = back_ref.shape
    logits = logit_ref[...]
    scores = [logits[:, k : k + 1] for k in range(2)]
    largest = jnp.maximum(scores[0], scores[1])
    powers = [jnp.exp(score - largest) for score in scores]
    whole = powers[0] + powers[1]
    slots = slot_ref[...]
    value = jnp.zeros((tokens, features), jnp.float32)
    done = 0
    for e in range(groups * count):
        block = back_ref[e // count, e % count]
        names = lax.broadcasted_iota(jnp.int32, (tokens, capacity), 1) + e * capacity
        for k in range(2):
            table = jnp.where(names == slots[:, k : k + 1], 1.0, 0.0).astype(jnp.bfloat16)
            picked = lax.dot_general(
                table, block, (((1,), (1,)), ((), ())), preferred_element_type=jnp.float32
            )
            value = value + picked * (powers[k] / whole)
        until = (e + 1) * len(pieces) // (groups * count)
        for n in range(done, until):
            load(n).wait()
            store(n).start()
        done = until
    out_ref[...] = value.astype(jnp.bfloat16)
    for n in range(len(pieces)):
        store(n).wait()


def finish(gate, up, down, back, slots, logits, features):
    parts = 4
    local_count, height, width = gate.shape
    count = 3 * local_count * parts
    hbm = pl.BlockSpec(memory_space=pl.ANY)
    vmem = pl.BlockSpec(memory_space=pltpu.VMEM)
    same = jax.ShapeDtypeStruct(gate.shape, gate.dtype)
    return pl.pallas_call(
        functools.partial(finish_kernel, parts),
        out_shape=(
            same, same, same, jax.ShapeDtypeStruct((slots.shape[0], features), jnp.bfloat16)
        ),
        in_specs=[hbm, hbm, hbm, vmem, vmem, vmem],
        out_specs=(hbm, hbm, hbm, vmem),
        scratch_shapes=[
            pltpu.VMEM((count, height // parts, width), jnp.bfloat16),
            pltpu.SemaphoreType.DMA((count,)),
            pltpu.SemaphoreType.DMA((count,)),
        ],
        compiler_params=pltpu.CompilerParams(vmem_limit_bytes=56 * 1024 * 1024),
        cost_estimate=pl.CostEstimate(
            flops=4 * slots.shape[0] * back.size, bytes_accessed=12 * gate.size, transcendentals=0
        ),
    )(gate, up, down, back, slots, logits)


def fused_device(
    hidden_states, norm_gain, gate_master, up_master, down_master, expert_ids, route_logits
):
    groups = lax.axis_size("tp")
    experts = gate_master.shape[0]
    local_count = experts // groups
    tokens, pieces = hidden_states.shape
    capacity = tokens // 2
    gain = norm_gain[:, None]
    earlier = (jnp.arange(tokens)[:, None] > jnp.arange(tokens)[None, :]).astype(jnp.bfloat16)
    named = expert_ids[:, :, None] == jnp.arange(experts, dtype=jnp.int32)[None, None, :]
    chosen = jnp.any(named, axis=1).astype(jnp.bfloat16)
    before = jnp.dot(earlier, chosen, preferred_element_type=jnp.float32)
    position = jnp.sum(jnp.where(named, before[:, None, :], 0.0), axis=2).astype(jnp.int32)
    slot_ids = expert_ids * capacity + position
    spots = jnp.where(chosen > 0, before, -1.0).T.reshape(groups, local_count, tokens)
    *firsts, everything, spots = exchange(
        gain, gate_master, up_master, down_master, hidden_states, spots, 0, 1
    )
    gate, up, down, ordered = serve(
        gain, gate_master, up_master, down_master, everything, spots, firsts, 1, 2
    )
    return finish(gate, up, down, ordered, slot_ids, route_logits, pieces)


def arrange(weights, groups, row_groups):
    experts, rows, columns = weights.shape
    blocks = row_groups // groups
    split = weights.reshape(experts // groups, groups, rows, blocks, columns // blocks)
    split = split.reshape(groups, experts // groups, rows, blocks, columns // blocks)
    return jnp.transpose(split, (0, 3, 1, 2, 4))


def regroup(moved, row_groups):
    return moved.reshape((row_groups,) + moved.shape[2:])


def settle(arrived):
    return arrived.reshape(arrived.shape[1], arrived.shape[2], arrived.shape[3])


def per_device(
    hidden_states, norm_gain, gate_master, up_master, down_master, expert_ids, route_logits
):
    groups = lax.axis_size("tp")
    row_groups = lax.axis_size("fs")
    whole_tiles = gate_master.shape[2] // (row_groups // groups) % 128 == 0
    lined = groups == 4 and row_groups == 8
    if whole_tiles and lined and gate_master.shape[0] == 2 * groups:
        return fused_device(
            hidden_states, norm_gain, gate_master, up_master, down_master, expert_ids, route_logits
        )
    experts = gate_master.shape[0]
    local_count = experts // groups
    tokens = hidden_states.shape[0]
    pieces = hidden_states.shape[1]
    model_width = pieces * row_groups
    capacity = tokens // 2
    scaled = norm_gain[None, :, None]
    gate_cast = arrange((scaled * gate_master).astype(jnp.bfloat16), groups, row_groups)
    up_cast = arrange((scaled * up_master).astype(jnp.bfloat16), groups, row_groups)
    down_cast = arrange(down_master.astype(jnp.bfloat16), groups, row_groups)
    sectioned = (
        lax.all_to_all(gate_cast, "tp", split_axis=0, concat_axis=0, tiled=True),
        lax.all_to_all(up_cast, "tp", split_axis=0, concat_axis=0, tiled=True),
        lax.all_to_all(down_cast, "tp", split_axis=0, concat_axis=0, tiled=True),
    )
    landed = (
        lax.all_to_all(
            regroup(sectioned[0], row_groups), "fs", split_axis=0, concat_axis=2, tiled=True
        ),
        lax.all_to_all(
            regroup(sectioned[1], row_groups), "fs", split_axis=0, concat_axis=2, tiled=True
        ),
        lax.all_to_all(
            regroup(sectioned[2], row_groups), "fs", split_axis=0, concat_axis=2, tiled=True
        ),
    )
    gate_serve, up_serve, down_serve = (settle(landed[0]), settle(landed[1]), settle(landed[2]))
    values = hidden_states.astype(jnp.float32)
    squares = lax.psum(jnp.sum(values * values, axis=1), "fs")
    normed = (values * lax.rsqrt(squares / model_width + EPSILON)[:, None]).astype(jnp.bfloat16)
    weights = jax.nn.softmax(route_logits, axis=1)
    chosen = (expert_ids[:, :, None] == jnp.arange(experts, dtype=jnp.int32)[None, None, :]).astype(
        jnp.int32
    )
    chosen = chosen.reshape(tokens * 2, experts)
    before = jnp.cumsum(chosen, axis=0) - chosen
    position = jnp.sum(before * chosen, axis=1)
    slot_ids = expert_ids.reshape(-1) * capacity + position
    slot_table = (
        slot_ids[None, :] == jnp.arange(experts * capacity, dtype=jnp.int32)[:, None]
    ).astype(jnp.bfloat16)
    dispatch = jnp.sum(slot_table.reshape(experts * capacity, tokens, 2), axis=2)
    whole_rows = lax.all_gather(normed, "fs", axis=1, tiled=True)
    packed = jnp.dot(dispatch, whole_rows, preferred_element_type=jnp.float32).astype(jnp.bfloat16)
    arrived = lax.all_to_all(
        packed.reshape(groups, local_count * capacity, model_width),
        "tp",
        split_axis=0,
        concat_axis=0,
        tiled=True,
    )
    arranged = arrived.reshape(groups, local_count, capacity, model_width)
    activations = []
    for expert_index in range(local_count):
        expert_rows = arranged[:, expert_index].reshape(groups * capacity, model_width)
        gate_pre = jnp.dot(
            expert_rows, gate_serve[expert_index], preferred_element_type=jnp.float32
        )
        up_pre = jnp.dot(expert_rows, up_serve[expert_index], preferred_element_type=jnp.float32)
        activations.append((jax.nn.silu(gate_pre) * up_pre).astype(jnp.bfloat16))
    stacked = jnp.stack(activations)
    summed = lax.psum_scatter(
        jnp.einsum("jdh,jsh->djs", down_serve, stacked, preferred_element_type=jnp.float32).astype(
            jnp.bfloat16
        ),
        "fs",
        scatter_dimension=0,
        tiled=True,
    )
    results = summed.reshape(pieces, local_count, groups, capacity)
    returned = lax.all_to_all(results, "tp", split_axis=2, concat_axis=1, tiled=True)
    flat_out = returned.reshape(pieces, experts * capacity)
    picked = jnp.take(flat_out, slot_ids, axis=1).reshape(pieces, tokens, 2).astype(jnp.float32)
    combined = jnp.sum(picked * weights[None, :, :], axis=2)
    return (gate_serve, up_serve, down_serve, jnp.transpose(combined).astype(jnp.bfloat16))


def solution(mesh):
    in_specs = (
        P("tp", "fs"),
        P("fs"),
        P(None, "fs", "tp"),
        P(None, "fs", "tp"),
        P(None, "fs", "tp"),
        P("tp", None),
        P("tp", None),
    )
    out_specs = (P("tp", None, "fs"), P("tp", None, "fs"), P("tp", None, "fs"), P("tp", "fs"))
    return jax.shard_map(
        per_device, mesh=mesh, in_specs=in_specs, out_specs=out_specs, check_vma=False
    )
```

```python
import functools

import jax
import jax.numpy as jnp
from jax import lax
from jax.experimental import pallas as pl
from jax.experimental.pallas import tpu as pltpu
from jax.sharding import PartitionSpec as P

EPSILON = 1e-06
SLOTS = 4
MESH = pl.DeviceIdType.MESH


def exchange_kernel(
    groups, row_groups, expert, units, gain_ref, gate_ref, up_ref, down_ref, own_ref, spot_ref,
    gate_out, up_out, down_out, all_out, spot_out, stage, cast, landed, load_sem,
    send_a, recv_a, send_b, recv_b, send_z, recv_z, send_y, recv_y, send_t, recv_t,
    send_s, recv_s, own_sem,
):
    me = lax.axis_index("tp")
    row = lax.axis_index("fs")
    blocks = row_groups // groups
    masters = (gate_ref, up_ref, down_ref)
    outs = (gate_out, up_out, down_out)
    local_count = gate_ref.shape[0] // groups
    rows, columns = gate_ref.shape[1:]
    width = columns // blocks
    strip = 16

    barrier = pltpu.get_barrier_semaphore()
    for step in range(1, groups):
        pl.semaphore_signal(
            barrier, inc=1, device_id={"tp": lax.rem(me + step, groups)}, device_id_type=MESH
        )
    for step in range(1, row_groups):
        pl.semaphore_signal(
            barrier, inc=1, device_id={"fs": lax.rem(row + step, row_groups)}, device_id_type=MESH
        )
    rest = [s for s in range(1, groups) if s != groups // 2]
    order = [groups // 2] + rest + [0]
    opening = [groups // 2, 0] + rest
    jobs = [(u, s) for u in range(len(units)) for s in (order if u else opening)]

    def load(n):
        u, s = jobs[n]
        w, start, size = units[u]
        number = lax.rem(me + s, groups) * local_count + expert
        return pltpu.make_async_copy(
            masters[w].at[number, pl.ds(start, size)],
            stage.at[n % SLOTS, pl.ds(0, size)],
            load_sem.at[n % SLOTS],
        )

    for n in range(SLOTS):
        load(n).start()
    pl.semaphore_wait(barrier, groups - 1 + row_groups - 1)

    def cast_at(u, s):
        w, start, size = units[u]
        return cast.at[w, s, pl.ds(start, size)]

    def landed_at(u, s):
        w, start, size = units[u]
        return landed.at[w, s - 1, pl.ds(start, size)]

    def first(u, s):
        return pltpu.make_async_remote_copy(
            src_ref=cast_at(u, s),
            dst_ref=landed_at(u, s),
            send_sem=send_a.at[u, s - 1],
            recv_sem=recv_a.at[u, s - 1],
            device_id={"tp": lax.rem(me + s, groups)},
            device_id_type=MESH,
        )

    def place(u, source):
        w, start, size = units[u]
        at = pl.ds(pl.multiple_of(source * rows + start, strip), size)
        return outs[w].at[at]

    def second(u, s, b):
        held = landed_at(u, s) if s else cast_at(u, 0)
        goal = lax.rem(me + groups - s, groups) * blocks + b
        piece = held.at[:, pl.ds(b * width, width)]
        remote = lambda: pltpu.make_async_remote_copy(
            src_ref=piece,
            dst_ref=place(u, row),
            send_sem=send_b.at[u, s * blocks + b],
            recv_sem=recv_b.at[u, row],
            device_id={"fs": goal},
            device_id_type=MESH,
        )
        local = lambda: pltpu.make_async_copy(piece, place(u, row), recv_b.at[u, row])
        return goal, remote, local

    def pass_on(u, s):
        for b in range(blocks):
            goal, remote, local = second(u, s, b)

            @pl.when(goal != row)
            def _():
                remote().start()

            @pl.when(goal == row)
            def _():
                local().start()

    def forward(u):
        for s in sorted(range(1, groups), key=lambda s: s == groups // 2):
            first(u, s).wait_recv()
            pass_on(u, s)

    side = lax.rem(row, 2)
    mate = row + 1 - 2 * side
    stack = row_groups // 2
    level = row // 2

    def block(k, y):
        which = side if y == 0 else 1 - side
        return lax.rem(level + stack - k, stack) * 2 + which

    def up_z(k):
        return pltpu.make_async_remote_copy(
            src_ref=own_ref,
            dst_ref=all_out.at[row, me],
            send_sem=send_z.at[k - 1],
            recv_sem=recv_z.at[k - 1],
            device_id={"fs": lax.rem(level + k, stack) * 2 + side},
            device_id_type=MESH,
        )

    def over_y(k):
        place = all_out.at[block(k, 0), me]
        return pltpu.make_async_remote_copy(
            src_ref=own_ref if k == 0 else place,
            dst_ref=place,
            send_sem=send_y.at[k],
            recv_sem=recv_y.at[k],
            device_id={"fs": mate},
            device_id_type=MESH,
        )

    def over_tp(k, y, s):
        place = all_out.at[block(k, y), me]
        return pltpu.make_async_remote_copy(
            src_ref=own_ref if k == 0 and y == 0 else place,
            dst_ref=place,
            send_sem=send_t.at[y * stack + k, s - 1],
            recv_sem=recv_t.at[y * stack + k, s - 1],
            device_id={"tp": lax.rem(me + s, groups)},
            device_id_type=MESH,
        )

    def spots_to(s):
        goal = lax.rem(me + s, groups)
        return pltpu.make_async_remote_copy(
            src_ref=spot_ref.at[goal],
            dst_ref=spot_out.at[me],
            send_sem=send_s.at[s - 1],
            recv_sem=recv_s.at[s - 1],
            device_id={"tp": goal},
            device_id_type=MESH,
        )

    own_kept = pltpu.make_async_copy(own_ref, all_out.at[row, me], own_sem.at[0])
    spot_kept = pltpu.make_async_copy(spot_ref.at[me], spot_out.at[me], own_sem.at[1])
    own_kept.start()
    spot_kept.start()
    for k in range(1, stack):
        up_z(k).start()
    over_y(0).start()
    for s in range(1, groups):
        spots_to(s).start()

    def near_blocks():
        for k in range(stack):
            if k:
                up_z(k).wait_recv()
                over_y(k).start()
            for s in range(1, groups):
                over_tp(k, 0, s).start()

    def far_blocks():
        for k in range(stack):
            over_y(k).wait_recv()
            for s in range(1, groups):
                over_tp(k, 1, s).start()

    tasks = {2: near_blocks, 4: far_blocks}
    for n, (u, s) in enumerate(jobs):
        w, start, size = units[u]
        load(n).wait()
        slot = n % SLOTS

        def convert(i, carry):
            at = pl.ds(pl.multiple_of(i * strip, strip), strip)
            value = stage[slot, at, :]
            if w < 2:
                gain = gain_ref[pl.ds(pl.multiple_of(start + i * strip, strip), strip), :]
                value = value * gain
            to = pl.ds(pl.multiple_of(start + i * strip, strip), strip)
            cast[w, s, to, :] = value.astype(jnp.bfloat16)
            return carry

        lax.fori_loop(0, size // strip, convert, 0)
        if n + SLOTS < len(jobs):
            load(n + SLOTS).start()
        if s == 0:
            pass_on(u, 0)
        else:
            first(u, s).start()
        if n + 1 == len(jobs) or jobs[n + 1][0] != u:
            if u >= 1:
                forward(u - 1)
            if u in tasks:
                tasks[u]()
    forward(len(units) - 1)
    own_kept.wait()
    spot_kept.wait()
    for k in range(stack):
        if k:
            up_z(k).wait_send()
        over_y(k).wait_send()
        for s in range(1, groups):
            for y in range(2):
                over_tp(k, y, s).wait()
    for s in range(1, groups):
        spots_to(s).wait()
    for u in range(len(units)):
        for s in range(groups):
            if s:
                first(u, s).wait_send()
            for b in range(blocks):
                goal, remote, local = second(u, s, b)

                @pl.when(goal != row)
                def _():
                    remote().wait_send()
        for source in range(row_groups):
            pltpu.make_async_copy(
                cast_at(u, 0).at[:, pl.ds(0, width)], place(u, source), recv_b.at[u, source]
            ).wait()


def exchange(gain, gate, up, down, hidden, spots, expert, collective):
    groups = lax.axis_size("tp")
    row_groups = lax.axis_size("fs")
    experts, rows, columns = gate.shape
    blocks = row_groups // groups
    width = columns // blocks
    eighth = rows // 8
    plan = [(0, 0, eighth), (0, eighth, 3 * eighth), (0, 4 * eighth, 4 * eighth)]
    plan += [(w, start, 4 * eighth) for w in (1, 2) for start in (0, 4 * eighth)]
    units = len(plan)
    height = 4 * eighth
    out = jax.ShapeDtypeStruct((rows * row_groups, width), jnp.bfloat16)
    hbm = pl.BlockSpec(memory_space=pl.ANY)
    stack = row_groups // 2
    vmem = pl.BlockSpec(memory_space=pltpu.VMEM)
    sent = 3 * rows * columns * 2 * groups
    dma = lambda *shape: pltpu.SemaphoreType.DMA(shape)
    return pl.pallas_call(
        functools.partial(exchange_kernel, groups, row_groups, expert, plan),
        out_shape=(
            out, out, out,
            jax.ShapeDtypeStruct((row_groups, groups) + hidden.shape, hidden.dtype),
            jax.ShapeDtypeStruct(spots.shape, spots.dtype),
        ),
        in_specs=[vmem, hbm, hbm, hbm, vmem, vmem],
        out_specs=(hbm,) * 5,
        scratch_shapes=[
            pltpu.VMEM((SLOTS, height, columns), jnp.float32),
            pltpu.VMEM((3, groups, rows, columns), jnp.bfloat16),
            pltpu.VMEM((3, groups - 1, rows, columns), jnp.bfloat16),
            dma(SLOTS), dma(units, groups - 1), dma(units, groups - 1),
            dma(units, row_groups), dma(units, row_groups),
            dma(stack - 1), dma(stack - 1), dma(stack), dma(stack),
            dma(2 * stack, groups - 1), dma(2 * stack, groups - 1),
            dma(groups - 1), dma(groups - 1), dma(2),
        ],
        compiler_params=pltpu.CompilerParams(
            collective_id=collective, has_side_effects=True, vmem_limit_bytes=62 * 1024 * 1024
        ),
        cost_estimate=pl.CostEstimate(
            flops=rows * columns, bytes_accessed=32 * sent, transcendentals=0
        ),
    )(gain, gate, up, down, hidden, spots)


def serve_kernel(
    groups, row_groups, expert, units, gain_ref, gate_ref, up_ref, down_ref, all_ref, spot_ref,
    gate_first, up_first, down_first,
    gate_out, up_out, down_out, back_out,
    stage, cast, landed, raw, rows_in, gate_w, up_w, down_w, act, partial,
    pair, to_near, near, to_far, far, total,
    load_sem, send_a, recv_a, send_b, recv_b, raw_sem, weight_sem, keep_sem,
    send_c, recv_c, send_d, recv_d, send_f, recv_f, send_e, recv_e, last_sem,
):
    me = lax.axis_index("tp")
    row = lax.axis_index("fs")
    blocks = row_groups // groups
    masters = (gate_ref, up_ref, down_ref)
    outs = (gate_out, up_out, down_out)
    firsts = (gate_first, up_first, down_first)
    held_w = (gate_w, up_w, down_w)
    local_count = gate_ref.shape[0] // groups
    rows, columns = gate_ref.shape[1:]
    width = columns // blocks
    tokens, model_width = raw.shape
    capacity = tokens // 2
    side = lax.rem(row, 2)
    mate = row + 1 - 2 * side
    stack = row_groups // 2
    level = row // 2
    strip = 16

    barrier = pltpu.get_barrier_semaphore()
    for step in range(1, groups):
        pl.semaphore_signal(
            barrier, inc=1, device_id={"tp": lax.rem(me + step, groups)}, device_id_type=MESH
        )
    for step in range(1, row_groups):
        pl.semaphore_signal(
            barrier, inc=1, device_id={"fs": lax.rem(row + step, row_groups)}, device_id_type=MESH
        )
    rest = [s for s in range(1, groups) if s != groups // 2]
    order = [groups // 2] + rest + [0]
    opening = [groups // 2, 0] + rest
    jobs = [(u, s) for u in range(len(units)) for s in (order if u else opening)]

    def load(n):
        u, s = jobs[n]
        w, start, size = units[u]
        number = lax.rem(me + s, groups) * local_count + expert
        return pltpu.make_async_copy(
            masters[w].at[number, pl.ds(start, size)],
            stage.at[n % SLOTS, pl.ds(0, size)],
            load_sem.at[n % SLOTS],
        )

    for n in range(SLOTS):
        load(n).start()
    pl.semaphore_wait(barrier, groups - 1 + row_groups - 1)

    def cast_at(u, s):
        w, start, size = units[u]
        return cast.at[w, s, pl.ds(start, size)]

    def landed_at(u, s):
        w, start, size = units[u]
        return landed.at[w, s - 1, pl.ds(start, size)]

    def first(u, s):
        return pltpu.make_async_remote_copy(
            src_ref=cast_at(u, s),
            dst_ref=landed_at(u, s),
            send_sem=send_a.at[u, s - 1],
            recv_sem=recv_a.at[u, s - 1],
            device_id={"tp": lax.rem(me + s, groups)},
            device_id_type=MESH,
        )

    def place(u, source):
        w, start, size = units[u]
        at = pl.ds(pl.multiple_of(source * rows + start, strip), size)
        return outs[w].at[expert, at]

    def second(u, s, b):
        held = landed_at(u, s) if s else cast_at(u, 0)
        goal = lax.rem(me + groups - s, groups) * blocks + b
        piece = held.at[:, pl.ds(b * width, width)]
        remote = lambda: pltpu.make_async_remote_copy(
            src_ref=piece,
            dst_ref=place(u, row),
            send_sem=send_b.at[u, s * blocks + b],
            recv_sem=recv_b.at[u, row],
            device_id={"fs": goal},
            device_id_type=MESH,
        )
        local = lambda: pltpu.make_async_copy(piece, place(u, row), recv_b.at[u, row])
        return goal, remote, local

    def pass_on(u, s):
        for b in range(blocks):
            goal, remote, local = second(u, s, b)

            @pl.when(goal != row)
            def _():
                remote().start()

            @pl.when(goal == row)
            def _():
                local().start()

    def forward(u):
        for s in sorted(range(1, groups), key=lambda s: s == groups // 2):
            first(u, s).wait_recv()
            pass_on(u, s)

    def arrived(u, source):
        pltpu.make_async_copy(
            cast_at(u, 0).at[:, pl.ds(0, width)], place(u, source), recv_b.at[u, source]
        ).wait()

    def pack(j):
        def one(g, carry):
            copies = [
                pltpu.make_async_copy(
                    all_ref.at[f, g],
                    raw.at[:, pl.ds(f * (model_width // row_groups), model_width // row_groups)],
                    raw_sem.at[f],
                )
                for f in range(row_groups)
            ]
            for copy in copies:
                copy.start()
            for copy in copies:
                copy.wait()
            spot = spot_ref[g, pl.ds(j, 1), :]
            slot = lax.broadcasted_iota(jnp.int32, (capacity, tokens), 0).astype(jnp.float32)
            table = jnp.where(slot == spot, 1.0, 0.0).astype(jnp.bfloat16)
            packed = jnp.dot(table, raw[...], preferred_element_type=jnp.float32)
            mean = jnp.mean(packed * packed, axis=1, keepdims=True)
            at = pl.ds(pl.multiple_of(g * capacity, capacity), capacity)
            rows_in[at, :] = (packed * lax.rsqrt(mean + EPSILON)).astype(jnp.bfloat16)
            return carry

        lax.fori_loop(0, groups, one, 0)

    def hidden():
        def one(t, carry):
            at = pl.ds(pl.multiple_of(t * capacity, capacity), capacity)
            value = rows_in[at, :]
            gate_pre = jnp.dot(value, gate_w[...], preferred_element_type=jnp.float32)
            up_pre = jnp.dot(value, up_w[...], preferred_element_type=jnp.float32)
            act[at, :] = (gate_pre / (1.0 + jnp.exp(-gate_pre)) * up_pre).astype(jnp.bfloat16)
            return carry

        lax.fori_loop(0, groups, one, 0)

    def lower(start, size):
        at = pl.ds(pl.multiple_of(start, strip), size)
        partial[at, :] = lax.dot_general(
            down_w[at, :], act[...], (((1,), (1,)), ((), ())), preferred_element_type=jnp.float32
        ).astype(jnp.bfloat16)

    def fetch(w, j):
        source = firsts[w] if j == 0 else outs[w].at[j]
        return pltpu.make_async_copy(source, held_w[w], weight_sem.at[w])

    def keep(w):
        return pltpu.make_async_copy(held_w[w], outs[w].at[0], keep_sem.at[w])

    def level_at(d):
        return lax.rem(level // 2 + d // 2, 2) * 2 + lax.rem(level + d, 2)

    lasts = [u for u in range(len(units)) if units[u][0] == 2]
    chunks = len(lasts)

    def span(c):
        return pl.ds(*units[lasts[c]][1:])

    def across(j, d, c):
        start, size = units[lasts[c]][1:]
        start = (level_at(d) * 2 + 1 - side) * rows + start
        return pltpu.make_async_remote_copy(
            src_ref=partial.at[pl.ds(pl.multiple_of(start, strip), size)],
            dst_ref=pair.at[j, d, span(c)],
            send_sem=send_c.at[j, d, c],
            recv_sem=recv_c.at[j, d, c],
            device_id={"fs": mate},
            device_id_type=MESH,
        )

    def along_near(j, d, c):
        return pltpu.make_async_remote_copy(
            src_ref=to_near.at[j, d - 1, span(c)],
            dst_ref=near.at[j, d - 1, span(c)],
            send_sem=send_d.at[j, d - 1, c],
            recv_sem=recv_d.at[j, d - 1, c],
            device_id={"fs": level_at(1) * 2 + side},
            device_id_type=MESH,
        )

    def along_far(j, c):
        return pltpu.make_async_remote_copy(
            src_ref=to_far.at[j, span(c)],
            dst_ref=far.at[j, span(c)],
            send_sem=send_f.at[j, c],
            recv_sem=recv_f.at[j, c],
            device_id={"fs": level_at(3) * 2 + side},
            device_id_type=MESH,
        )

    def back(j, s, c):
        goal = lax.rem(me + s, groups)
        columns = pl.ds(pl.multiple_of(goal * capacity, capacity), capacity)
        return pltpu.make_async_remote_copy(
            src_ref=total.at[j, span(c), columns],
            dst_ref=back_out.at[me, j, span(c)],
            send_sem=send_e.at[j, s - 1, c],
            recv_sem=recv_e.at[j, s - 1, c],
            device_id={"tp": goal},
            device_id_type=MESH,
        )

    def kept(j, c):
        columns = pl.ds(pl.multiple_of(me * capacity, capacity), capacity)
        return pltpu.make_async_copy(
            total.at[j, span(c), columns], back_out.at[me, j, span(c)], last_sem.at[j, c]
        )

    def sum_into(j, d, c, target, others):
        start, size = units[lasts[c]][1:]
        base = (level_at(d) * 2 + side) * rows

        def add(i, carry):
            at = pl.ds(pl.multiple_of(start + i * strip, strip), strip)
            mine = pl.ds(pl.multiple_of(base + start + i * strip, strip), strip)
            value = partial[mine, :].astype(jnp.float32) + pair[j, d, at, :].astype(jnp.float32)
            for other in others:
                value = value + other[at, :].astype(jnp.float32)
            target[at, :] = value.astype(jnp.bfloat16)
            return carry

        lax.fori_loop(0, size // strip, add, 0)

    def to_level(j, d, c):
        across(j, d, c).wait_recv()
        sum_into(j, d, c, to_near.at[j, d - 1], ())
        along_near(j, d, c).start()

    def cross_over(j, c):
        across(j, 3, c).wait_recv()
        along_near(j, 2, c).wait_recv()
        sum_into(j, 3, c, to_far.at[j], (near.at[j, 1],))
        along_far(j, c).start()

    def settle_sum(j, c):
        across(j, 0, c).wait_recv()
        along_near(j, 1, c).wait_recv()
        along_far(j, c).wait_recv()
        sum_into(j, 0, c, total.at[j], (near.at[j, 0], far.at[j]))
        for s in range(1, groups):
            back(j, s, c).start()
        kept(j, c).start()

    def after_0():
        for w in range(len(masters)):
            fetch(w, 0).start()
        pack(0)

    def after_1():
        for w in range(2):
            fetch(w, 0).wait()
            keep(w).start()
        hidden()

    def after_2():
        fetch(2, 0).wait()
        keep(2).start()

        def one(r, carry):
            lower(r * rows, rows)
            return carry

        lax.fori_loop(0, row_groups, one, 0)
        for c in range(chunks):
            for d in range(stack):
                across(0, d, c).start()

    def after_3():
        for c in range(chunks):
            to_level(0, 2, c)
            to_level(0, 1, c)

    def after_4():
        for c in range(chunks):
            cross_over(0, c)

    tasks = {1: after_0, 2: after_1, 3: after_2, 4: after_3, 5: after_4}
    held_unit = len(units) - 1

    for n, (u, s) in enumerate(jobs):
        w, start, size = units[u]
        load(n).wait()
        slot = n % SLOTS

        def convert(i, carry):
            at = pl.ds(pl.multiple_of(i * strip, strip), strip)
            value = stage[slot, at, :]
            if w < 2:
                gain = gain_ref[pl.ds(pl.multiple_of(start + i * strip, strip), strip), :]
                value = value * gain
            to = pl.ds(pl.multiple_of(start + i * strip, strip), strip)
            cast[w, s, to, :] = value.astype(jnp.bfloat16)
            return carry

        lax.fori_loop(0, size // strip, convert, 0)
        if n + SLOTS < len(jobs):
            load(n + SLOTS).start()
        if s == 0:
            if u != held_unit:
                pass_on(u, 0)
        else:
            first(u, s).start()
        if n + 1 == len(jobs) or jobs[n + 1][0] != u:
            if u >= 1:
                forward(u - 1)
            if u in tasks:
                tasks[u]()
    pack(1)
    for w in range(2):
        keep(w).wait()
        for u in range(len(units)):
            if units[u][0] == w:
                for source in range(row_groups):
                    arrived(u, source)
        fetch(w, expert).start()
    for w in range(2):
        fetch(w, expert).wait()
    hidden()
    keep(2).wait()
    for c in range(chunks):
        settle_sum(0, c)
        for d in range(stack):
            across(0, d, c).wait_send()

    def piece(d, i, c):
        source = level_at(d) * 2 + lax.rem(side + 1 + i, 2)
        start, size = units[lasts[c]][1:]
        at = pl.ds(pl.multiple_of(source * rows + start, strip), size)
        copy = pltpu.make_async_copy(outs[2].at[expert, at], down_w.at[at], raw_sem.at[i])
        return source, copy

    def level_product(d, c):
        for i in range(2):
            source, copy = piece(d, i, c)
            arrived(lasts[c], source)
            copy.start()
        for i in range(2):
            piece(d, i, c)[1].wait()

        def one(i, carry):
            start, size = units[lasts[c]][1:]
            lower((level_at(d) * 2 + lax.rem(side + 1 + i, 2)) * rows + start, size)
            return carry

        lax.fori_loop(0, 2, one, 0)
        across(1, d, c).start()

    for c in range(chunks):
        for d in range(stack):
            level_product(d, c)
        to_level(1, 2, c)
        to_level(1, 1, c)
        if c == 0:
            pass_on(held_unit, 0)
            forward(held_unit)
        cross_over(1, c)
    for c in range(chunks):
        settle_sum(1, c)
    for c in range(chunks):
        for d in range(stack):
            across(1, d, c).wait_send()
        for j in range(2):
            for d in (1, 2):
                along_near(j, d, c).wait_send()
            along_far(j, c).wait_send()
            kept(j, c).wait()
            for s in range(1, groups):
                back(j, s, c).wait()
    for u in range(len(units)):
        for s in range(groups):
            if s:
                first(u, s).wait_send()
            for b in range(blocks):
                goal, remote, local = second(u, s, b)

                @pl.when(goal != row)
                def _():
                    remote().wait_send()


def serve(gain, gate, up, down, everything, spots, firsts, expert, collective):
    groups = lax.axis_size("tp")
    row_groups = lax.axis_size("fs")
    experts, rows, columns = gate.shape
    blocks = row_groups // groups
    width = columns // blocks
    model_width = rows * row_groups
    tokens = spots.shape[2]
    capacity = tokens // 2
    slots = groups * capacity
    eighth = rows // 8
    plan = [(0, 0, eighth), (0, eighth, 3 * eighth), (0, 4 * eighth, 4 * eighth)]
    plan += [(1, 0, 4 * eighth), (1, 4 * eighth, 4 * eighth)]
    plan += [(2, 0, 4 * eighth), (2, 4 * eighth, 2 * eighth), (2, 6 * eighth, 2 * eighth)]
    units = len(plan)
    chunks = 3
    height = 4 * eighth
    stack = row_groups // 2
    out = jax.ShapeDtypeStruct((experts // groups, model_width, width), jnp.bfloat16)
    hbm = pl.BlockSpec(memory_space=pl.ANY)
    vmem = pl.BlockSpec(memory_space=pltpu.VMEM)
    sent = 3 * rows * columns * 2 * groups
    weight = pltpu.VMEM((model_width, width), jnp.bfloat16)
    dma = lambda *shape: pltpu.SemaphoreType.DMA(shape)
    return pl.pallas_call(
        functools.partial(serve_kernel, groups, row_groups, expert, plan),
        out_shape=(
            out, out, out,
            jax.ShapeDtypeStruct((groups, 2, rows, capacity), jnp.bfloat16),
        ),
        in_specs=[vmem, hbm, hbm, hbm, hbm, vmem, hbm, hbm, hbm],
        out_specs=(hbm,) * 4,
        scratch_shapes=[
            pltpu.VMEM((SLOTS, height, columns), jnp.float32),
            pltpu.VMEM((3, groups, rows, columns), jnp.bfloat16),
            pltpu.VMEM((3, groups - 1, rows, columns), jnp.bfloat16),
            pltpu.VMEM((tokens, model_width), jnp.bfloat16),
            pltpu.VMEM((slots, model_width), jnp.bfloat16),
            weight, weight, weight,
            pltpu.VMEM((slots, width), jnp.bfloat16),
            pltpu.VMEM((model_width, slots), jnp.bfloat16),
            pltpu.VMEM((2, stack, rows, slots), jnp.bfloat16),
            pltpu.VMEM((2, 2, rows, slots), jnp.bfloat16),
            pltpu.VMEM((2, 2, rows, slots), jnp.bfloat16),
            pltpu.VMEM((2, rows, slots), jnp.bfloat16),
            pltpu.VMEM((2, rows, slots), jnp.bfloat16),
            pltpu.VMEM((2, rows, slots), jnp.bfloat16),
            dma(SLOTS), dma(units, groups - 1), dma(units, groups - 1),
            dma(units, row_groups), dma(units, row_groups),
            dma(row_groups), dma(3), dma(3),
            dma(2, stack, chunks), dma(2, stack, chunks),
            dma(2, 2, chunks), dma(2, 2, chunks), dma(2, chunks), dma(2, chunks),
            dma(2, groups - 1, chunks), dma(2, groups - 1, chunks), dma(2, chunks),
        ],
        compiler_params=pltpu.CompilerParams(
            collective_id=collective, has_side_effects=True, vmem_limit_bytes=62 * 1024 * 1024
        ),
        cost_estimate=pl.CostEstimate(
            flops=12 * slots * model_width * width, bytes_accessed=32 * sent, transcendentals=0
        ),
    )(gain, gate, up, down, everything, spots, *firsts)


def finish_kernel(
    parts, gate_ref, up_ref, down_ref, back_ref, slot_ref, logit_ref,
    gate_out, up_out, down_out, out_ref, held, load_sem, store_sem,
):
    sources = (gate_ref, up_ref, down_ref)
    goals = (gate_out, up_out, down_out)
    local_count, height, width = gate_ref.shape
    part = height // parts
    pieces = [
        (w, j, pl.ds(p * part, part))
        for w in range(3) for j in range(local_count) for p in range(parts)
    ]

    def load(n):
        w, j, at = pieces[n]
        return pltpu.make_async_copy(sources[w].at[j, at], held.at[n], load_sem.at[n])

    def store(n):
        w, j, at = pieces[n]
        return pltpu.make_async_copy(held.at[n], goals[w].at[j, at], store_sem.at[n])

    for n in range(len(pieces)):
        load(n).start()
    tokens, features = out_ref.shape
    groups, count, _, capacity = back_ref.shape
    logits = logit_ref[...]
    scores = [logits[k : k + 1, :] for k in range(2)]
    largest = jnp.maximum(scores[0], scores[1])
    powers = [jnp.exp(score - largest) for score in scores]
    whole = powers[0] + powers[1]
    slots = slot_ref[...]
    value = jnp.zeros((features, tokens), jnp.float32)
    done = 0
    for e in range(groups * count):
        block = back_ref[e // count, e % count]
        names = lax.broadcasted_iota(jnp.int32, (capacity, tokens), 0) + e * capacity
        for k in range(2):
            table = jnp.where(names == slots[k : k + 1, :], 1.0, 0.0).astype(jnp.bfloat16)
            picked = jnp.dot(block, table, preferred_element_type=jnp.float32)
            value = value + picked * (powers[k] / whole)
        until = (e + 1) * len(pieces) // (groups * count)
        for n in range(done, until):
            load(n).wait()
            store(n).start()
        done = until
    out_ref[...] = jnp.transpose(value).astype(jnp.bfloat16)
    for n in range(len(pieces)):
        store(n).wait()


def finish(gate, up, down, back, slots, logits, features):
    parts = 4
    local_count, height, width = gate.shape
    count = 3 * local_count * parts
    hbm = pl.BlockSpec(memory_space=pl.ANY)
    vmem = pl.BlockSpec(memory_space=pltpu.VMEM)
    same = jax.ShapeDtypeStruct(gate.shape, gate.dtype)
    return pl.pallas_call(
        functools.partial(finish_kernel, parts),
        out_shape=(
            same, same, same, jax.ShapeDtypeStruct((slots.shape[1], features), jnp.bfloat16)
        ),
        in_specs=[hbm, hbm, hbm, vmem, vmem, vmem],
        out_specs=(hbm, hbm, hbm, vmem),
        scratch_shapes=[
            pltpu.VMEM((count, height // parts, width), jnp.bfloat16),
            pltpu.SemaphoreType.DMA((count,)),
            pltpu.SemaphoreType.DMA((count,)),
        ],
        compiler_params=pltpu.CompilerParams(vmem_limit_bytes=56 * 1024 * 1024),
        cost_estimate=pl.CostEstimate(
            flops=4 * slots.shape[1] * back.size, bytes_accessed=12 * gate.size, transcendentals=0
        ),
    )(gate, up, down, back, slots, logits)


def fused_device(
    hidden_states, norm_gain, gate_master, up_master, down_master, expert_ids, route_logits
):
    groups = lax.axis_size("tp")
    experts = gate_master.shape[0]
    local_count = experts // groups
    tokens, pieces = hidden_states.shape
    capacity = tokens // 2
    gain = norm_gain[:, None]
    earlier = (jnp.arange(tokens)[:, None] > jnp.arange(tokens)[None, :]).astype(jnp.bfloat16)
    named = expert_ids[:, :, None] == jnp.arange(experts, dtype=jnp.int32)[None, None, :]
    chosen = jnp.any(named, axis=1).astype(jnp.bfloat16)
    before = jnp.dot(earlier, chosen, preferred_element_type=jnp.float32)
    position = jnp.sum(jnp.where(named, before[:, None, :], 0.0), axis=2).astype(jnp.int32)
    slot_ids = expert_ids * capacity + position
    spots = jnp.where(chosen > 0, before, -1.0).T.reshape(groups, local_count, tokens)
    *firsts, everything, spots = exchange(
        gain, gate_master, up_master, down_master, hidden_states, spots, 0, 1
    )
    gate, up, down, ordered = serve(
        gain, gate_master, up_master, down_master, everything, spots, firsts, 1, 2
    )
    return finish(gate, up, down, ordered, slot_ids.T, route_logits.T, pieces)


def arrange(weights, groups, row_groups):
    experts, rows, columns = weights.shape
    blocks = row_groups // groups
    split = weights.reshape(experts // groups, groups, rows, blocks, columns // blocks)
    split = split.reshape(groups, experts // groups, rows, blocks, columns // blocks)
    return jnp.transpose(split, (0, 3, 1, 2, 4))


def regroup(moved, row_groups):
    return moved.reshape((row_groups,) + moved.shape[2:])


def settle(arrived):
    return arrived.reshape(arrived.shape[1], arrived.shape[2], arrived.shape[3])


def per_device(
    hidden_states, norm_gain, gate_master, up_master, down_master, expert_ids, route_logits
):
    groups = lax.axis_size("tp")
    row_groups = lax.axis_size("fs")
    whole_tiles = gate_master.shape[2] // (row_groups // groups) % 128 == 0
    lined = groups == 4 and row_groups == 8
    if whole_tiles and lined and gate_master.shape[0] == 2 * groups:
        return fused_device(
            hidden_states, norm_gain, gate_master, up_master, down_master, expert_ids, route_logits
        )
    experts = gate_master.shape[0]
    local_count = experts // groups
    tokens = hidden_states.shape[0]
    pieces = hidden_states.shape[1]
    model_width = pieces * row_groups
    capacity = tokens // 2
    scaled = norm_gain[None, :, None]
    gate_cast = arrange((scaled * gate_master).astype(jnp.bfloat16), groups, row_groups)
    up_cast = arrange((scaled * up_master).astype(jnp.bfloat16), groups, row_groups)
    down_cast = arrange(down_master.astype(jnp.bfloat16), groups, row_groups)
    sectioned = (
        lax.all_to_all(gate_cast, "tp", split_axis=0, concat_axis=0, tiled=True),
        lax.all_to_all(up_cast, "tp", split_axis=0, concat_axis=0, tiled=True),
        lax.all_to_all(down_cast, "tp", split_axis=0, concat_axis=0, tiled=True),
    )
    landed = (
        lax.all_to_all(
            regroup(sectioned[0], row_groups), "fs", split_axis=0, concat_axis=2, tiled=True
        ),
        lax.all_to_all(
            regroup(sectioned[1], row_groups), "fs", split_axis=0, concat_axis=2, tiled=True
        ),
        lax.all_to_all(
            regroup(sectioned[2], row_groups), "fs", split_axis=0, concat_axis=2, tiled=True
        ),
    )
    gate_serve, up_serve, down_serve = (settle(landed[0]), settle(landed[1]), settle(landed[2]))
    values = hidden_states.astype(jnp.float32)
    squares = lax.psum(jnp.sum(values * values, axis=1), "fs")
    normed = (values * lax.rsqrt(squares / model_width + EPSILON)[:, None]).astype(jnp.bfloat16)
    weights = jax.nn.softmax(route_logits, axis=1)
    chosen = (expert_ids[:, :, None] == jnp.arange(experts, dtype=jnp.int32)[None, None, :]).astype(
        jnp.int32
    )
    chosen = chosen.reshape(tokens * 2, experts)
    before = jnp.cumsum(chosen, axis=0) - chosen
    position = jnp.sum(before * chosen, axis=1)
    slot_ids = expert_ids.reshape(-1) * capacity + position
    slot_table = (
        slot_ids[None, :] == jnp.arange(experts * capacity, dtype=jnp.int32)[:, None]
    ).astype(jnp.bfloat16)
    dispatch = jnp.sum(slot_table.reshape(experts * capacity, tokens, 2), axis=2)
    whole_rows = lax.all_gather(normed, "fs", axis=1, tiled=True)
    packed = jnp.dot(dispatch, whole_rows, preferred_element_type=jnp.float32).astype(jnp.bfloat16)
    arrived = lax.all_to_all(
        packed.reshape(groups, local_count * capacity, model_width),
        "tp",
        split_axis=0,
        concat_axis=0,
        tiled=True,
    )
    arranged = arrived.reshape(groups, local_count, capacity, model_width)
    activations = []
    for expert_index in range(local_count):
        expert_rows = arranged[:, expert_index].reshape(groups * capacity, model_width)
        gate_pre = jnp.dot(
            expert_rows, gate_serve[expert_index], preferred_element_type=jnp.float32
        )
        up_pre = jnp.dot(expert_rows, up_serve[expert_index], preferred_element_type=jnp.float32)
        activations.append((jax.nn.silu(gate_pre) * up_pre).astype(jnp.bfloat16))
    stacked = jnp.stack(activations)
    summed = lax.psum_scatter(
        jnp.einsum("jdh,jsh->djs", down_serve, stacked, preferred_element_type=jnp.float32).astype(
            jnp.bfloat16
        ),
        "fs",
        scatter_dimension=0,
        tiled=True,
    )
    results = summed.reshape(pieces, local_count, groups, capacity)
    returned = lax.all_to_all(results, "tp", split_axis=2, concat_axis=1, tiled=True)
    flat_out = returned.reshape(pieces, experts * capacity)
    picked = jnp.take(flat_out, slot_ids, axis=1).reshape(pieces, tokens, 2).astype(jnp.float32)
    combined = jnp.sum(picked * weights[None, :, :], axis=2)
    return (gate_serve, up_serve, down_serve, jnp.transpose(combined).astype(jnp.bfloat16))


def solution(mesh):
    in_specs = (
        P("tp", "fs"),
        P("fs"),
        P(None, "fs", "tp"),
        P(None, "fs", "tp"),
        P(None, "fs", "tp"),
        P("tp", None),
        P("tp", None),
    )
    out_specs = (P("tp", None, "fs"), P("tp", None, "fs"), P("tp", None, "fs"), P("tp", "fs"))
    return jax.shard_map(
        per_device, mesh=mesh, in_specs=in_specs, out_specs=out_specs, check_vma=False
    )
```

```python
import functools

import jax
import jax.numpy as jnp
from jax import lax
from jax.experimental import pallas as pl
from jax.experimental.pallas import tpu as pltpu
from jax.sharding import PartitionSpec as P

EPSILON = 1e-06
SLOTS = 4
MESH = pl.DeviceIdType.MESH


def exchange_kernel(
    groups, row_groups, expert, units, gain_ref, gate_ref, up_ref, down_ref, own_ref, spot_ref,
    gate_out, up_out, down_out, all_out, spot_out, stage, cast, landed, load_sem,
    send_a, recv_a, send_b, recv_b, send_z, recv_z, send_y, recv_y, send_t, recv_t,
    send_s, recv_s, own_sem,
):
    me = lax.axis_index("tp")
    row = lax.axis_index("fs")
    blocks = row_groups // groups
    masters = (gate_ref, up_ref, down_ref)
    outs = (gate_out, up_out, down_out)
    local_count = gate_ref.shape[0] // groups
    rows, columns = gate_ref.shape[1:]
    width = columns // blocks
    strip = 16

    barrier = pltpu.get_barrier_semaphore()
    for step in range(1, groups):
        pl.semaphore_signal(
            barrier, inc=1, device_id={"tp": lax.rem(me + step, groups)}, device_id_type=MESH
        )
    for step in range(1, row_groups):
        pl.semaphore_signal(
            barrier, inc=1, device_id={"fs": lax.rem(row + step, row_groups)}, device_id_type=MESH
        )
    rest = [s for s in range(1, groups) if s != groups // 2]
    order = [groups // 2] + rest + [0]
    opening = [groups // 2, 0] + rest
    jobs = [(u, s) for u in range(len(units)) for s in (order if u else opening)]

    def load(n):
        u, s = jobs[n]
        w, start, size = units[u]
        number = lax.rem(me + s, groups) * local_count + expert
        return pltpu.make_async_copy(
            masters[w].at[number, pl.ds(start, size)],
            stage.at[n % SLOTS, pl.ds(0, size)],
            load_sem.at[n % SLOTS],
        )

    for n in range(SLOTS):
        load(n).start()
    pl.semaphore_wait(barrier, groups - 1 + row_groups - 1)

    def cast_at(u, s):
        w, start, size = units[u]
        return cast.at[w, s, pl.ds(start, size)]

    def landed_at(u, s):
        w, start, size = units[u]
        return landed.at[w, s - 1, pl.ds(start, size)]

    def first(u, s):
        return pltpu.make_async_remote_copy(
            src_ref=cast_at(u, s),
            dst_ref=landed_at(u, s),
            send_sem=send_a.at[u, s - 1],
            recv_sem=recv_a.at[u, s - 1],
            device_id={"tp": lax.rem(me + s, groups)},
            device_id_type=MESH,
        )

    def place(u, source):
        w, start, size = units[u]
        at = pl.ds(pl.multiple_of(source * rows + start, strip), size)
        return outs[w].at[at]

    def second(u, s, b):
        held = landed_at(u, s) if s else cast_at(u, 0)
        goal = lax.rem(me + groups - s, groups) * blocks + b
        piece = held.at[:, pl.ds(b * width, width)]
        remote = lambda: pltpu.make_async_remote_copy(
            src_ref=piece,
            dst_ref=place(u, row),
            send_sem=send_b.at[u, s * blocks + b],
            recv_sem=recv_b.at[u, row],
            device_id={"fs": goal},
            device_id_type=MESH,
        )
        local = lambda: pltpu.make_async_copy(piece, place(u, row), recv_b.at[u, row])
        return goal, remote, local

    def pass_on(u, s):
        for b in range(blocks):
            goal, remote, local = second(u, s, b)

            @pl.when(goal != row)
            def _():
                remote().start()

            @pl.when(goal == row)
            def _():
                local().start()

    def forward(u):
        for s in sorted(range(1, groups), key=lambda s: s == groups // 2):
            first(u, s).wait_recv()
            pass_on(u, s)

    side = lax.rem(row, 2)
    mate = row + 1 - 2 * side
    stack = row_groups // 2
    level = row // 2

    def block(k, y):
        which = side if y == 0 else 1 - side
        return lax.rem(level + stack - k, stack) * 2 + which

    def up_z(k):
        return pltpu.make_async_remote_copy(
            src_ref=own_ref,
            dst_ref=all_out.at[row, me],
            send_sem=send_z.at[k - 1],
            recv_sem=recv_z.at[k - 1],
            device_id={"fs": lax.rem(level + k, stack) * 2 + side},
            device_id_type=MESH,
        )

    def over_y(k):
        place = all_out.at[block(k, 0), me]
        return pltpu.make_async_remote_copy(
            src_ref=own_ref if k == 0 else place,
            dst_ref=place,
            send_sem=send_y.at[k],
            recv_sem=recv_y.at[k],
            device_id={"fs": mate},
            device_id_type=MESH,
        )

    def over_tp(k, y, s):
        place = all_out.at[block(k, y), me]
        return pltpu.make_async_remote_copy(
            src_ref=own_ref if k == 0 and y == 0 else place,
            dst_ref=place,
            send_sem=send_t.at[y * stack + k, s - 1],
            recv_sem=recv_t.at[y * stack + k, s - 1],
            device_id={"tp": lax.rem(me + s, groups)},
            device_id_type=MESH,
        )

    def spots_to(s):
        goal = lax.rem(me + s, groups)
        return pltpu.make_async_remote_copy(
            src_ref=spot_ref.at[goal],
            dst_ref=spot_out.at[me],
            send_sem=send_s.at[s - 1],
            recv_sem=recv_s.at[s - 1],
            device_id={"tp": goal},
            device_id_type=MESH,
        )

    own_kept = pltpu.make_async_copy(own_ref, all_out.at[row, me], own_sem.at[0])
    spot_kept = pltpu.make_async_copy(spot_ref.at[me], spot_out.at[me], own_sem.at[1])
    own_kept.start()
    spot_kept.start()
    for k in range(1, stack):
        up_z(k).start()
    over_y(0).start()
    for s in range(1, groups):
        spots_to(s).start()

    def near_blocks():
        for k in range(stack):
            if k:
                up_z(k).wait_recv()
                over_y(k).start()
            for s in range(1, groups):
                over_tp(k, 0, s).start()

    def far_blocks():
        for k in range(stack):
            over_y(k).wait_recv()
            for s in range(1, groups):
                over_tp(k, 1, s).start()

    tasks = {2: near_blocks, 4: far_blocks}
    for n, (u, s) in enumerate(jobs):
        w, start, size = units[u]
        load(n).wait()
        slot = n % SLOTS

        def convert(i, carry):
            at = pl.ds(pl.multiple_of(i * strip, strip), strip)
            value = stage[slot, at, :]
            if w < 2:
                gain = gain_ref[pl.ds(pl.multiple_of(start + i * strip, strip), strip), :]
                value = value * gain
            to = pl.ds(pl.multiple_of(start + i * strip, strip), strip)
            cast[w, s, to, :] = value.astype(jnp.bfloat16)
            return carry

        lax.fori_loop(0, size // strip, convert, 0)
        if n + SLOTS < len(jobs):
            load(n + SLOTS).start()
        if s == 0:
            pass_on(u, 0)
        else:
            first(u, s).start()
        if n + 1 == len(jobs) or jobs[n + 1][0] != u:
            if u >= 1:
                forward(u - 1)
            if u in tasks:
                tasks[u]()
    forward(len(units) - 1)
    own_kept.wait()
    spot_kept.wait()
    for k in range(stack):
        if k:
            up_z(k).wait_send()
        over_y(k).wait_send()
        for s in range(1, groups):
            for y in range(2):
                over_tp(k, y, s).wait()
    for s in range(1, groups):
        spots_to(s).wait()
    for u in range(len(units)):
        for s in range(groups):
            if s:
                first(u, s).wait_send()
            for b in range(blocks):
                goal, remote, local = second(u, s, b)

                @pl.when(goal != row)
                def _():
                    remote().wait_send()
        for source in range(row_groups):
            pltpu.make_async_copy(
                cast_at(u, 0).at[:, pl.ds(0, width)], place(u, source), recv_b.at[u, source]
            ).wait()


def exchange(gain, gate, up, down, hidden, spots, expert, collective):
    groups = lax.axis_size("tp")
    row_groups = lax.axis_size("fs")
    experts, rows, columns = gate.shape
    blocks = row_groups // groups
    width = columns // blocks
    eighth = rows // 8
    plan = [(0, 0, eighth), (0, eighth, 3 * eighth), (0, 4 * eighth, 4 * eighth)]
    plan += [(w, start, 4 * eighth) for w in (1, 2) for start in (0, 4 * eighth)]
    units = len(plan)
    height = 4 * eighth
    out = jax.ShapeDtypeStruct((rows * row_groups, width), jnp.bfloat16)
    hbm = pl.BlockSpec(memory_space=pl.ANY)
    stack = row_groups // 2
    vmem = pl.BlockSpec(memory_space=pltpu.VMEM)
    sent = 3 * rows * columns * 2 * groups
    dma = lambda *shape: pltpu.SemaphoreType.DMA(shape)
    return pl.pallas_call(
        functools.partial(exchange_kernel, groups, row_groups, expert, plan),
        out_shape=(
            out, out, out,
            jax.ShapeDtypeStruct((row_groups, groups) + hidden.shape, hidden.dtype),
            jax.ShapeDtypeStruct(spots.shape, spots.dtype),
        ),
        in_specs=[vmem, hbm, hbm, hbm, vmem, vmem],
        out_specs=(hbm,) * 5,
        scratch_shapes=[
            pltpu.VMEM((SLOTS, height, columns), jnp.float32),
            pltpu.VMEM((3, groups, rows, columns), jnp.bfloat16),
            pltpu.VMEM((3, groups - 1, rows, columns), jnp.bfloat16),
            dma(SLOTS), dma(units, groups - 1), dma(units, groups - 1),
            dma(units, row_groups), dma(units, row_groups),
            dma(stack - 1), dma(stack - 1), dma(stack), dma(stack),
            dma(2 * stack, groups - 1), dma(2 * stack, groups - 1),
            dma(groups - 1), dma(groups - 1), dma(2),
        ],
        compiler_params=pltpu.CompilerParams(
            collective_id=collective, has_side_effects=True, vmem_limit_bytes=62 * 1024 * 1024
        ),
        cost_estimate=pl.CostEstimate(
            flops=rows * columns, bytes_accessed=32 * sent, transcendentals=0
        ),
    )(gain, gate, up, down, hidden, spots)


def serve_kernel(
    groups, row_groups, expert, units, gain_ref, gate_ref, up_ref, down_ref, all_ref, spot_ref,
    gate_first, up_first, down_first,
    gate_out, up_out, down_out, back_out,
    stage, cast, landed, raw, rows_in, gate_w, up_w, down_w, act, partial,
    pair, to_near, near, to_far, far, total,
    load_sem, send_a, recv_a, send_b, recv_b, raw_sem, weight_sem, keep_sem,
    send_c, recv_c, send_d, recv_d, send_f, recv_f, send_e, recv_e, last_sem,
):
    me = lax.axis_index("tp")
    row = lax.axis_index("fs")
    blocks = row_groups // groups
    masters = (gate_ref, up_ref, down_ref)
    outs = (gate_out, up_out, down_out)
    firsts = (gate_first, up_first, down_first)
    held_w = (gate_w, up_w, down_w)
    local_count = gate_ref.shape[0] // groups
    rows, columns = gate_ref.shape[1:]
    width = columns // blocks
    tokens, model_width = raw.shape
    capacity = tokens // 2
    side = lax.rem(row, 2)
    mate = row + 1 - 2 * side
    stack = row_groups // 2
    level = row // 2
    strip = 16

    barrier = pltpu.get_barrier_semaphore()
    for step in range(1, groups):
        pl.semaphore_signal(
            barrier, inc=1, device_id={"tp": lax.rem(me + step, groups)}, device_id_type=MESH
        )
    for step in range(1, row_groups):
        pl.semaphore_signal(
            barrier, inc=1, device_id={"fs": lax.rem(row + step, row_groups)}, device_id_type=MESH
        )
    rest = [s for s in range(1, groups) if s != groups // 2]
    order = [groups // 2] + rest + [0]
    opening = [groups // 2, 0] + rest
    jobs = [(u, s) for u in range(len(units)) for s in (order if u else opening)]

    def load(n):
        u, s = jobs[n]
        w, start, size = units[u]
        number = lax.rem(me + s, groups) * local_count + expert
        return pltpu.make_async_copy(
            masters[w].at[number, pl.ds(start, size)],
            stage.at[n % SLOTS, pl.ds(0, size)],
            load_sem.at[n % SLOTS],
        )

    for n in range(SLOTS):
        load(n).start()
    pl.semaphore_wait(barrier, groups - 1 + row_groups - 1)

    def cast_at(u, s):
        w, start, size = units[u]
        return cast.at[w, s, pl.ds(start, size)]

    def landed_at(u, s):
        w, start, size = units[u]
        return landed.at[w, s - 1, pl.ds(start, size)]

    def first(u, s):
        return pltpu.make_async_remote_copy(
            src_ref=cast_at(u, s),
            dst_ref=landed_at(u, s),
            send_sem=send_a.at[u, s - 1],
            recv_sem=recv_a.at[u, s - 1],
            device_id={"tp": lax.rem(me + s, groups)},
            device_id_type=MESH,
        )

    def place(u, source):
        w, start, size = units[u]
        at = pl.ds(pl.multiple_of(source * rows + start, strip), size)
        return outs[w].at[expert, at]

    def second(u, s, b):
        held = landed_at(u, s) if s else cast_at(u, 0)
        goal = lax.rem(me + groups - s, groups) * blocks + b
        piece = held.at[:, pl.ds(b * width, width)]
        remote = lambda: pltpu.make_async_remote_copy(
            src_ref=piece,
            dst_ref=place(u, row),
            send_sem=send_b.at[u, s * blocks + b],
            recv_sem=recv_b.at[u, row],
            device_id={"fs": goal},
            device_id_type=MESH,
        )
        local = lambda: pltpu.make_async_copy(piece, place(u, row), recv_b.at[u, row])
        return goal, remote, local

    def pass_on(u, s):
        for b in range(blocks):
            goal, remote, local = second(u, s, b)

            @pl.when(goal != row)
            def _():
                remote().start()

            @pl.when(goal == row)
            def _():
                local().start()

    def forward(u):
        for s in sorted(range(1, groups), key=lambda s: s == groups // 2):
            first(u, s).wait_recv()
            pass_on(u, s)

    def arrived(u, source):
        pltpu.make_async_copy(
            cast_at(u, 0).at[:, pl.ds(0, width)], place(u, source), recv_b.at[u, source]
        ).wait()

    def pack(j):
        def one(g, carry):
            copies = [
                pltpu.make_async_copy(
                    all_ref.at[f, g],
                    raw.at[:, pl.ds(f * (model_width // row_groups), model_width // row_groups)],
                    raw_sem.at[f],
                )
                for f in range(row_groups)
            ]
            for copy in copies:
                copy.start()
            for copy in copies:
                copy.wait()
            spot = spot_ref[g, pl.ds(j, 1), :]
            slot = lax.broadcasted_iota(jnp.int32, (capacity, tokens), 0).astype(jnp.float32)
            table = jnp.where(slot == spot, 1.0, 0.0).astype(jnp.bfloat16)
            packed = jnp.dot(table, raw[...], preferred_element_type=jnp.float32)
            mean = jnp.mean(packed * packed, axis=1, keepdims=True)
            at = pl.ds(pl.multiple_of(g * capacity, capacity), capacity)
            rows_in[at, :] = (packed * lax.rsqrt(mean + EPSILON)).astype(jnp.bfloat16)
            return carry

        lax.fori_loop(0, groups, one, 0)

    def hidden():
        def one(t, carry):
            at = pl.ds(pl.multiple_of(t * capacity, capacity), capacity)
            value = rows_in[at, :]
            gate_pre = jnp.dot(value, gate_w[...], preferred_element_type=jnp.float32)
            up_pre = jnp.dot(value, up_w[...], preferred_element_type=jnp.float32)
            act[at, :] = (gate_pre / (1.0 + jnp.exp(-gate_pre)) * up_pre).astype(jnp.bfloat16)
            return carry

        lax.fori_loop(0, groups, one, 0)

    def lower(start, size):
        at = pl.ds(pl.multiple_of(start, strip), size)
        partial[at, :] = lax.dot_general(
            down_w[at, :], act[...], (((1,), (1,)), ((), ())), preferred_element_type=jnp.float32
        ).astype(jnp.bfloat16)

    def fetch(w, j):
        source = firsts[w] if j == 0 else outs[w].at[j]
        return pltpu.make_async_copy(source, held_w[w], weight_sem.at[w])

    def keep(w):
        return pltpu.make_async_copy(held_w[w], outs[w].at[0], keep_sem.at[w])

    def level_at(d):
        return lax.rem(level // 2 + d // 2, 2) * 2 + lax.rem(level + d, 2)

    lasts = [u for u in range(len(units)) if units[u][0] == 2]
    chunks = len(lasts)

    def span(c):
        return pl.ds(*units[lasts[c]][1:])

    def across(j, d, c):
        start, size = units[lasts[c]][1:]
        start = (level_at(d) * 2 + 1 - side) * rows + start
        return pltpu.make_async_remote_copy(
            src_ref=partial.at[pl.ds(pl.multiple_of(start, strip), size)],
            dst_ref=pair.at[j, d, span(c)],
            send_sem=send_c.at[j, d, c],
            recv_sem=recv_c.at[j, d, c],
            device_id={"fs": mate},
            device_id_type=MESH,
        )

    def along_near(j, d, c):
        return pltpu.make_async_remote_copy(
            src_ref=to_near.at[j, d - 1, span(c)],
            dst_ref=near.at[j, d - 1, span(c)],
            send_sem=send_d.at[j, d - 1, c],
            recv_sem=recv_d.at[j, d - 1, c],
            device_id={"fs": level_at(1) * 2 + side},
            device_id_type=MESH,
        )

    def along_far(j, c):
        return pltpu.make_async_remote_copy(
            src_ref=to_far.at[j, span(c)],
            dst_ref=far.at[j, span(c)],
            send_sem=send_f.at[j, c],
            recv_sem=recv_f.at[j, c],
            device_id={"fs": level_at(3) * 2 + side},
            device_id_type=MESH,
        )

    def back(j, s, c):
        goal = lax.rem(me + s, groups)
        columns = pl.ds(pl.multiple_of(goal * capacity, capacity), capacity)
        return pltpu.make_async_remote_copy(
            src_ref=total.at[j, span(c), columns],
            dst_ref=back_out.at[me, j, span(c)],
            send_sem=send_e.at[j, s - 1, c],
            recv_sem=recv_e.at[j, s - 1, c],
            device_id={"tp": goal},
            device_id_type=MESH,
        )

    def kept(j, c):
        columns = pl.ds(pl.multiple_of(me * capacity, capacity), capacity)
        return pltpu.make_async_copy(
            total.at[j, span(c), columns], back_out.at[me, j, span(c)], last_sem.at[j, c]
        )

    def sum_into(j, d, c, target, others):
        start, size = units[lasts[c]][1:]
        base = (level_at(d) * 2 + side) * rows

        def add(i, carry):
            at = pl.ds(pl.multiple_of(start + i * strip, strip), strip)
            mine = pl.ds(pl.multiple_of(base + start + i * strip, strip), strip)
            value = partial[mine, :].astype(jnp.float32) + pair[j, d, at, :].astype(jnp.float32)
            for other in others:
                value = value + other[at, :].astype(jnp.float32)
            target[at, :] = value.astype(jnp.bfloat16)
            return carry

        lax.fori_loop(0, size // strip, add, 0)

    def to_level(j, d, c):
        across(j, d, c).wait_recv()
        sum_into(j, d, c, to_near.at[j, d - 1], ())
        along_near(j, d, c).start()

    def cross_over(j, c):
        across(j, 3, c).wait_recv()
        along_near(j, 2, c).wait_recv()
        sum_into(j, 3, c, to_far.at[j], (near.at[j, 1],))
        along_far(j, c).start()

    def settle_sum(j, c):
        across(j, 0, c).wait_recv()
        along_near(j, 1, c).wait_recv()
        along_far(j, c).wait_recv()
        sum_into(j, 0, c, total.at[j], (near.at[j, 0], far.at[j]))
        for s in range(1, groups):
            back(j, s, c).start()
        kept(j, c).start()

    def after_0():
        for w in range(len(masters)):
            fetch(w, 0).start()
        pack(0)

    def after_1():
        for w in range(2):
            fetch(w, 0).wait()
            keep(w).start()
        hidden()

    def after_2():
        fetch(2, 0).wait()
        keep(2).start()

        def one(r, carry):
            lower(r * rows, rows)
            return carry

        lax.fori_loop(0, row_groups, one, 0)
        for c in range(chunks):
            for d in range(stack):
                across(0, d, c).start()

    def after_3():
        for c in range(chunks):
            to_level(0, 2, c)
            to_level(0, 1, c)

    def after_4():
        for c in range(chunks):
            cross_over(0, c)

    tasks = {1: after_0, 2: after_1, 3: after_2, 4: after_3, 5: after_4}
    held_unit = len(units) - 1

    for n, (u, s) in enumerate(jobs):
        w, start, size = units[u]
        load(n).wait()
        slot = n % SLOTS

        def convert(i, carry):
            at = pl.ds(pl.multiple_of(i * strip, strip), strip)
            value = stage[slot, at, :]
            if w < 2:
                gain = gain_ref[pl.ds(pl.multiple_of(start + i * strip, strip), strip), :]
                value = value * gain
            to = pl.ds(pl.multiple_of(start + i * strip, strip), strip)
            cast[w, s, to, :] = value.astype(jnp.bfloat16)
            return carry

        lax.fori_loop(0, size // strip, convert, 0)
        if n + SLOTS < len(jobs):
            load(n + SLOTS).start()
        if s == 0:
            if u != held_unit:
                pass_on(u, 0)
        else:
            first(u, s).start()
        if n + 1 == len(jobs) or jobs[n + 1][0] != u:
            if u >= 1:
                forward(u - 1)
            if u in tasks:
                tasks[u]()
    pack(1)
    for w in range(2):
        keep(w).wait()
        for u in range(len(units)):
            if units[u][0] == w:
                for source in range(row_groups):
                    arrived(u, source)
        fetch(w, expert).start()
    for w in range(2):
        fetch(w, expert).wait()
    hidden()
    keep(2).wait()
    for c in range(chunks):
        settle_sum(0, c)
        for d in range(stack):
            across(0, d, c).wait_send()

    def piece(d, i, c):
        source = level_at(d) * 2 + lax.rem(side + 1 + i, 2)
        start, size = units[lasts[c]][1:]
        at = pl.ds(pl.multiple_of(source * rows + start, strip), size)
        copy = pltpu.make_async_copy(outs[2].at[expert, at], down_w.at[at], raw_sem.at[i])
        return source, copy

    def level_product(d, c):
        for i in range(2):
            source, copy = piece(d, i, c)
            arrived(lasts[c], source)
            copy.start()
        for i in range(2):
            piece(d, i, c)[1].wait()

        def one(i, carry):
            start, size = units[lasts[c]][1:]
            lower((level_at(d) * 2 + lax.rem(side + 1 + i, 2)) * rows + start, size)
            return carry

        lax.fori_loop(0, 2, one, 0)
        across(1, d, c).start()

    for c in range(chunks):
        for d in range(stack):
            level_product(d, c)
        to_level(1, 2, c)
        to_level(1, 1, c)
        if c == 0:
            pass_on(held_unit, 0)
            forward(held_unit)
        cross_over(1, c)
    for c in range(chunks):
        settle_sum(1, c)
    for c in range(chunks):
        for d in range(stack):
            across(1, d, c).wait_send()
        for j in range(2):
            for d in (1, 2):
                along_near(j, d, c).wait_send()
            along_far(j, c).wait_send()
            kept(j, c).wait()
            for s in range(1, groups):
                back(j, s, c).wait()
    for u in range(len(units)):
        for s in range(groups):
            if s:
                first(u, s).wait_send()
            for b in range(blocks):
                goal, remote, local = second(u, s, b)

                @pl.when(goal != row)
                def _():
                    remote().wait_send()


def serve(gain, gate, up, down, everything, spots, firsts, expert, collective):
    groups = lax.axis_size("tp")
    row_groups = lax.axis_size("fs")
    experts, rows, columns = gate.shape
    blocks = row_groups // groups
    width = columns // blocks
    model_width = rows * row_groups
    tokens = spots.shape[2]
    capacity = tokens // 2
    slots = groups * capacity
    eighth = rows // 8
    plan = [(0, 0, eighth), (0, eighth, 3 * eighth), (0, 4 * eighth, 4 * eighth)]
    plan += [(1, 0, 4 * eighth), (1, 4 * eighth, 4 * eighth)]
    plan += [(2, 0, 3 * eighth), (2, 3 * eighth, 3 * eighth), (2, 6 * eighth, 2 * eighth)]
    units = len(plan)
    chunks = 3
    height = 4 * eighth
    stack = row_groups // 2
    out = jax.ShapeDtypeStruct((experts // groups, model_width, width), jnp.bfloat16)
    hbm = pl.BlockSpec(memory_space=pl.ANY)
    vmem = pl.BlockSpec(memory_space=pltpu.VMEM)
    sent = 3 * rows * columns * 2 * groups
    weight = pltpu.VMEM((model_width, width), jnp.bfloat16)
    dma = lambda *shape: pltpu.SemaphoreType.DMA(shape)
    return pl.pallas_call(
        functools.partial(serve_kernel, groups, row_groups, expert, plan),
        out_shape=(
            out, out, out,
            jax.ShapeDtypeStruct((groups, 2, rows, capacity), jnp.bfloat16),
        ),
        in_specs=[vmem, hbm, hbm, hbm, hbm, vmem, hbm, hbm, hbm],
        out_specs=(hbm,) * 4,
        scratch_shapes=[
            pltpu.VMEM((SLOTS, height, columns), jnp.float32),
            pltpu.VMEM((3, groups, rows, columns), jnp.bfloat16),
            pltpu.VMEM((3, groups - 1, rows, columns), jnp.bfloat16),
            pltpu.VMEM((tokens, model_width), jnp.bfloat16),
            pltpu.VMEM((slots, model_width), jnp.bfloat16),
            weight, weight, weight,
            pltpu.VMEM((slots, width), jnp.bfloat16),
            pltpu.VMEM((model_width, slots), jnp.bfloat16),
            pltpu.VMEM((2, stack, rows, slots), jnp.bfloat16),
            pltpu.VMEM((2, 2, rows, slots), jnp.bfloat16),
            pltpu.VMEM((2, 2, rows, slots), jnp.bfloat16),
            pltpu.VMEM((2, rows, slots), jnp.bfloat16),
            pltpu.VMEM((2, rows, slots), jnp.bfloat16),
            pltpu.VMEM((2, rows, slots), jnp.bfloat16),
            dma(SLOTS), dma(units, groups - 1), dma(units, groups - 1),
            dma(units, row_groups), dma(units, row_groups),
            dma(row_groups), dma(3), dma(3),
            dma(2, stack, chunks), dma(2, stack, chunks),
            dma(2, 2, chunks), dma(2, 2, chunks), dma(2, chunks), dma(2, chunks),
            dma(2, groups - 1, chunks), dma(2, groups - 1, chunks), dma(2, chunks),
        ],
        compiler_params=pltpu.CompilerParams(
            collective_id=collective, has_side_effects=True, vmem_limit_bytes=62 * 1024 * 1024
        ),
        cost_estimate=pl.CostEstimate(
            flops=12 * slots * model_width * width, bytes_accessed=32 * sent, transcendentals=0
        ),
    )(gain, gate, up, down, everything, spots, *firsts)


def finish_kernel(
    parts, gate_ref, up_ref, down_ref, back_ref, slot_ref, logit_ref,
    gate_out, up_out, down_out, out_ref, held, load_sem, store_sem,
):
    sources = (gate_ref, up_ref, down_ref)
    goals = (gate_out, up_out, down_out)
    local_count, height, width = gate_ref.shape
    part = height // parts
    pieces = [
        (w, j, pl.ds(p * part, part))
        for w in range(3) for j in range(local_count) for p in range(parts)
    ]

    def load(n):
        w, j, at = pieces[n]
        return pltpu.make_async_copy(sources[w].at[j, at], held.at[n], load_sem.at[n])

    def store(n):
        w, j, at = pieces[n]
        return pltpu.make_async_copy(held.at[n], goals[w].at[j, at], store_sem.at[n])

    for n in range(len(pieces)):
        load(n).start()
    tokens, features = out_ref.shape
    groups, count, _, capacity = back_ref.shape
    logits = logit_ref[...]
    scores = [logits[k : k + 1, :] for k in range(2)]
    largest = jnp.maximum(scores[0], scores[1])
    powers = [jnp.exp(score - largest) for score in scores]
    whole = powers[0] + powers[1]
    slots = slot_ref[...]
    value = jnp.zeros((features, tokens), jnp.float32)
    done = 0
    for e in range(groups * count):
        block = back_ref[e // count, e % count]
        names = lax.broadcasted_iota(jnp.int32, (capacity, tokens), 0) + e * capacity
        for k in range(2):
            table = jnp.where(names == slots[k : k + 1, :], 1.0, 0.0).astype(jnp.bfloat16)
            picked = jnp.dot(block, table, preferred_element_type=jnp.float32)
            value = value + picked * (powers[k] / whole)
        until = (e + 1) * len(pieces) // (groups * count)
        for n in range(done, until):
            load(n).wait()
            store(n).start()
        done = until
    out_ref[...] = jnp.transpose(value).astype(jnp.bfloat16)
    for n in range(len(pieces)):
        store(n).wait()


def finish(gate, up, down, back, slots, logits, features):
    parts = 4
    local_count, height, width = gate.shape
    count = 3 * local_count * parts
    hbm = pl.BlockSpec(memory_space=pl.ANY)
    vmem = pl.BlockSpec(memory_space=pltpu.VMEM)
    same = jax.ShapeDtypeStruct(gate.shape, gate.dtype)
    return pl.pallas_call(
        functools.partial(finish_kernel, parts),
        out_shape=(
            same, same, same, jax.ShapeDtypeStruct((slots.shape[1], features), jnp.bfloat16)
        ),
        in_specs=[hbm, hbm, hbm, vmem, vmem, vmem],
        out_specs=(hbm, hbm, hbm, vmem),
        scratch_shapes=[
            pltpu.VMEM((count, height // parts, width), jnp.bfloat16),
            pltpu.SemaphoreType.DMA((count,)),
            pltpu.SemaphoreType.DMA((count,)),
        ],
        compiler_params=pltpu.CompilerParams(vmem_limit_bytes=56 * 1024 * 1024),
        cost_estimate=pl.CostEstimate(
            flops=4 * slots.shape[1] * back.size, bytes_accessed=12 * gate.size, transcendentals=0
        ),
    )(gate, up, down, back, slots, logits)


def fused_device(
    hidden_states, norm_gain, gate_master, up_master, down_master, expert_ids, route_logits
):
    groups = lax.axis_size("tp")
    experts = gate_master.shape[0]
    local_count = experts // groups
    tokens, pieces = hidden_states.shape
    capacity = tokens // 2
    gain = norm_gain[:, None]
    earlier = (jnp.arange(tokens)[:, None] > jnp.arange(tokens)[None, :]).astype(jnp.bfloat16)
    named = expert_ids[:, :, None] == jnp.arange(experts, dtype=jnp.int32)[None, None, :]
    chosen = jnp.any(named, axis=1).astype(jnp.bfloat16)
    before = jnp.dot(earlier, chosen, preferred_element_type=jnp.float32)
    position = jnp.sum(jnp.where(named, before[:, None, :], 0.0), axis=2).astype(jnp.int32)
    slot_ids = expert_ids * capacity + position
    spots = jnp.where(chosen > 0, before, -1.0).T.reshape(groups, local_count, tokens)
    *firsts, everything, spots = exchange(
        gain, gate_master, up_master, down_master, hidden_states, spots, 0, 1
    )
    gate, up, down, ordered = serve(
        gain, gate_master, up_master, down_master, everything, spots, firsts, 1, 2
    )
    return finish(gate, up, down, ordered, slot_ids.T, route_logits.T, pieces)


def arrange(weights, groups, row_groups):
    experts, rows, columns = weights.shape
    blocks = row_groups // groups
    split = weights.reshape(experts // groups, groups, rows, blocks, columns // blocks)
    split = split.reshape(groups, experts // groups, rows, blocks, columns // blocks)
    return jnp.transpose(split, (0, 3, 1, 2, 4))


def regroup(moved, row_groups):
    return moved.reshape((row_groups,) + moved.shape[2:])


def settle(arrived):
    return arrived.reshape(arrived.shape[1], arrived.shape[2], arrived.shape[3])


def per_device(
    hidden_states, norm_gain, gate_master, up_master, down_master, expert_ids, route_logits
):
    groups = lax.axis_size("tp")
    row_groups = lax.axis_size("fs")
    whole_tiles = gate_master.shape[2] // (row_groups // groups) % 128 == 0
    lined = groups == 4 and row_groups == 8
    if whole_tiles and lined and gate_master.shape[0] == 2 * groups:
        return fused_device(
            hidden_states, norm_gain, gate_master, up_master, down_master, expert_ids, route_logits
        )
    experts = gate_master.shape[0]
    local_count = experts // groups
    tokens = hidden_states.shape[0]
    pieces = hidden_states.shape[1]
    model_width = pieces * row_groups
    capacity = tokens // 2
    scaled = norm_gain[None, :, None]
    gate_cast = arrange((scaled * gate_master).astype(jnp.bfloat16), groups, row_groups)
    up_cast = arrange((scaled * up_master).astype(jnp.bfloat16), groups, row_groups)
    down_cast = arrange(down_master.astype(jnp.bfloat16), groups, row_groups)
    sectioned = (
        lax.all_to_all(gate_cast, "tp", split_axis=0, concat_axis=0, tiled=True),
        lax.all_to_all(up_cast, "tp", split_axis=0, concat_axis=0, tiled=True),
        lax.all_to_all(down_cast, "tp", split_axis=0, concat_axis=0, tiled=True),
    )
    landed = (
        lax.all_to_all(
            regroup(sectioned[0], row_groups), "fs", split_axis=0, concat_axis=2, tiled=True
        ),
        lax.all_to_all(
            regroup(sectioned[1], row_groups), "fs", split_axis=0, concat_axis=2, tiled=True
        ),
        lax.all_to_all(
            regroup(sectioned[2], row_groups), "fs", split_axis=0, concat_axis=2, tiled=True
        ),
    )
    gate_serve, up_serve, down_serve = (settle(landed[0]), settle(landed[1]), settle(landed[2]))
    values = hidden_states.astype(jnp.float32)
    squares = lax.psum(jnp.sum(values * values, axis=1), "fs")
    normed = (values * lax.rsqrt(squares / model_width + EPSILON)[:, None]).astype(jnp.bfloat16)
    weights = jax.nn.softmax(route_logits, axis=1)
    chosen = (expert_ids[:, :, None] == jnp.arange(experts, dtype=jnp.int32)[None, None, :]).astype(
        jnp.int32
    )
    chosen = chosen.reshape(tokens * 2, experts)
    before = jnp.cumsum(chosen, axis=0) - chosen
    position = jnp.sum(before * chosen, axis=1)
    slot_ids = expert_ids.reshape(-1) * capacity + position
    slot_table = (
        slot_ids[None, :] == jnp.arange(experts * capacity, dtype=jnp.int32)[:, None]
    ).astype(jnp.bfloat16)
    dispatch = jnp.sum(slot_table.reshape(experts * capacity, tokens, 2), axis=2)
    whole_rows = lax.all_gather(normed, "fs", axis=1, tiled=True)
    packed = jnp.dot(dispatch, whole_rows, preferred_element_type=jnp.float32).astype(jnp.bfloat16)
    arrived = lax.all_to_all(
        packed.reshape(groups, local_count * capacity, model_width),
        "tp",
        split_axis=0,
        concat_axis=0,
        tiled=True,
    )
    arranged = arrived.reshape(groups, local_count, capacity, model_width)
    activations = []
    for expert_index in range(local_count):
        expert_rows = arranged[:, expert_index].reshape(groups * capacity, model_width)
        gate_pre = jnp.dot(
            expert_rows, gate_serve[expert_index], preferred_element_type=jnp.float32
        )
        up_pre = jnp.dot(expert_rows, up_serve[expert_index], preferred_element_type=jnp.float32)
        activations.append((jax.nn.silu(gate_pre) * up_pre).astype(jnp.bfloat16))
    stacked = jnp.stack(activations)
    summed = lax.psum_scatter(
        jnp.einsum("jdh,jsh->djs", down_serve, stacked, preferred_element_type=jnp.float32).astype(
            jnp.bfloat16
        ),
        "fs",
        scatter_dimension=0,
        tiled=True,
    )
    results = summed.reshape(pieces, local_count, groups, capacity)
    returned = lax.all_to_all(results, "tp", split_axis=2, concat_axis=1, tiled=True)
    flat_out = returned.reshape(pieces, experts * capacity)
    picked = jnp.take(flat_out, slot_ids, axis=1).reshape(pieces, tokens, 2).astype(jnp.float32)
    combined = jnp.sum(picked * weights[None, :, :], axis=2)
    return (gate_serve, up_serve, down_serve, jnp.transpose(combined).astype(jnp.bfloat16))


def solution(mesh):
    in_specs = (
        P("tp", "fs"),
        P("fs"),
        P(None, "fs", "tp"),
        P(None, "fs", "tp"),
        P(None, "fs", "tp"),
        P("tp", None),
        P("tp", None),
    )
    out_specs = (P("tp", None, "fs"), P("tp", None, "fs"), P("tp", None, "fs"), P("tp", "fs"))
    return jax.shard_map(
        per_device, mesh=mesh, in_specs=in_specs, out_specs=out_specs, check_vma=False
    )
```
